32 devices in a mesh: ep: 8 (over z, core), tp: 4 (over y, x).
Axes of the slice: x: 2, y: 2, z: 4, core: 2. Of those that a mesh axis runs over, the one named last changes fastest.
Arguments:
- receptance: bfloat16 [2048, 2048], P('ep', 'tp'), may hold values from -6 to 6
- key_in: bfloat16 [2048, 2048], P('ep', 'tp'), may hold values from -6 to 6
- value_in: bfloat16 [2048, 2048], P('ep', 'tp'), may hold values from -6 to 6
- decay_in: bfloat16 [2048, 2048], P('ep', 'tp'), may hold values from -16 to 2
- rate_in: bfloat16 [2048, 2048], P('ep', 'tp'), may hold values from -12 to 4
- norm_gain: float32 [2048], P('tp'), may hold values from 0.1 to 1.9
- out_weight: bfloat16 [2048, 4096], P('tp'), may hold values from -0.125 to 0.125
- moe_in: bfloat16 [1024, 4096], P('ep'), may hold values from -6 to 6
- ffn_gain: float32 [4096], replicated, may hold values from 0.1 to 1.9
- routes: int32 [1024, 4], P('ep'), may hold values from 0 to 7, all different within a row; in each aligned block of 128 rows (0 to 127, 128 to 255, ...) at most 80 rows name the same one
- route_weights: float32 [1024, 4], P('ep'), may hold values from 0.2 to 1
- gate_weight: bfloat16 [8, 4096, 1024], P('ep', None, 'tp'), may hold values from -0.09375 to 0.09375
- up_weight: bfloat16 [8, 4096, 1024], P('ep', None, 'tp'), may hold values from -0.09375 to 0.09375
- down_weight: bfloat16 [8, 1024, 4096], P('ep', None, 'tp'), may hold values from -0.1875 to 0.1875
Outputs:
- mixer_out: bfloat16 [2048, 4096], P(('ep', 'tp'))
- moe_out: bfloat16 [1024, 4096], P('ep', 'tp')
The draws below stay inside these ranges and needn't reach their ends.
Inputs may be any that keep to these rules, and one draw needn't show every extreme that they name: `routes`: A row names 4 different experts. Among the 128 rows that one index of ep holds, no expert is named by more than 80 rows, and in every draw some expert is named by exactly 80 of them.
All inputs are finite; a program needn't handle non-finite values.
Results may differ from the reference program's by a relative error of at most 0.025.
Values may be sent and summed in bfloat16 or wider, within the bound.
A program may use at most 64 MiB of HBM per device.

```python
import math
import jax
import jax.numpy as jnp
import numpy as np
from jax import lax

D = 4096
HEADS = 32
HD = 64
FE = 1024
TOPK = 4
TOK_DEV = 256
R_DEV = 128
WIDTH = 2048
TOKENS = 2048
MOE_ROWS = 1024
EXPERTS = 8
CAP = 80
N_EP = 8
N_TP = 4


def slow_heads(key):
    chance = 0.5
    return jax.random.uniform(jax.random.fold_in(key, 11), (HEADS,)) < chance


def span_offsets(key, salt, reach):
    span_count = TOKENS // TOK_DEV
    offsets = jax.random.uniform(jax.random.fold_in(key, salt), (span_count, HEADS), jnp.float32, -reach, reach)
    return jnp.repeat(offsets, TOK_DEV, axis=0)[:, :, None]


def jitter(key, salt, spread):
    shape = (TOKENS, HEADS, HD)
    return jax.random.normal(jax.random.fold_in(key, salt), shape, jnp.float32) * spread


def draw_decay_in(key, part):
    slow = slow_heads(key)
    level = jnp.where(slow, math.log(0.5 / TOKENS) + 0.5, math.log(1.0 / 40.0) + 0.5).astype(jnp.float32)
    values = level[None, :, None] + span_offsets(key, 12, 1.0) + jitter(key, 13, 0.5)
    return jnp.clip(values, -16.0, 2.0).reshape(TOKENS, HEADS * HD).astype(jnp.bfloat16)


def draw_rate_in(key, part):
    slow = slow_heads(key)
    level = jnp.where(slow, math.log(0.5 * HD / TOKENS), 0.0).astype(jnp.float32)
    spread = jnp.where(slow, 0.5, 1.0).astype(jnp.float32)[None, :, None]
    values = level[None, :, None] + span_offsets(key, 14, 0.7) + jitter(key, 15, 1.0) * spread
    return jnp.clip(values, -12.0, 4.0).reshape(TOKENS, HEADS * HD).astype(jnp.bfloat16)


def block_levels(rng, extent, split, low, high):
    loudness, own = 1.0, jax.random.fold_in(rng, 6)
    for axis_at, parts in split:
        heights = jnp.exp(jax.random.uniform(jax.random.fold_in(own, axis_at), (parts,), jnp.float32, low / len(split), high / len(split)))
        loudness = loudness * jnp.repeat(heights, extent[axis_at] // parts).reshape([-1 if axis == axis_at else 1 for axis in range(len(extent))])
    return loudness


def routed_block(stream_key, own, number, rows, number_of, top, bound, slope):
    sequence = jax.random.permutation(stream_key, number_of)
    heavy_load, common = shares(number_of, rows * top, bound, slope, True), shares(number_of, rows * top, bound, slope, False)
    places = jnp.arange(number_of)

    def named(sizes, rotation):
        used = int((sizes > 0).sum())
        fixed = max(1, used // 4)
        moved = fixed + (places - fixed + rotation * (used - fixed)) % max(1, number_of - fixed)
        return jnp.zeros((number_of,), jnp.int32).at[sequence[jnp.where(places < fixed, places, moved)]].set(jnp.asarray(sizes, jnp.int32))

    sizes = jnp.where(number % 4 == 0, named(heavy_load, number // 4), named(common, number - number // 4 - 1))
    mixed = jax.random.permutation(jax.random.fold_in(own, 3), number_of)
    giver, sink = mixed[0:number_of // 2 * 2:2], mixed[1:number_of // 2 * 2:2]
    margin = jnp.minimum(sizes[giver] - 1, bound - sizes[sink]) // 2
    margin = jnp.where((giver == sequence[0]) | (sink == sequence[0]) | (sizes[sink] == 0), 0, jnp.maximum(margin, 0))
    moved = jax.random.randint(jax.random.fold_in(own, 4), (number_of // 2,), 0, 1 << 20) % (margin + 1)
    sizes = sizes.at[giver].add(-moved).at[sink].add(moved)
    members = jnp.searchsorted(jnp.cumsum(sizes), jnp.arange(rows * top), side="right").astype(jnp.int32)
    table = members.reshape(top, rows).T
    table = table[jax.random.permutation(jax.random.fold_in(own, 1), rows)]
    rotation = jax.random.randint(jax.random.fold_in(own, 2), (rows, 1), 0, top)
    return jnp.take_along_axis(table, (jnp.arange(top)[None, :] + rotation) % top, axis=1)


def shares(count, total, limit, slope, full):
    weights = [(1 << 20) // math.isqrt(rank ** slope) + 1 for rank in range(1, count + 1)]
    largest = limit if full else min(limit, max(-(-total // count), total * weights[0] // sum(weights)))
    least = 1 if total - largest >= count - 1 else 0
    given, surplus = [largest] + [least] * (count - 1), total - largest - least * (count - 1)
    while surplus > 0:
        movable = [i for i in range(1, count) if given[i] < largest] or [i for i in range(1, count) if given[i] < limit]
        pool, remaining = sum([weights[i] for i in movable]), surplus
        for i in movable:
            addition = min(limit - given[i], max(1, remaining * weights[i] // pool), surplus)
            given[i] = given[i] + addition
            surplus = surplus - addition
    return np.array(given)


def scatter_about(rng, dims, width, most, cuts=(), held_as=jnp.bfloat16):
    values = jax.random.normal(rng, dims, jnp.float32) * width
    if len(cuts) > 0:
        values = block_levels(rng, dims, cuts, -0.22, 0.18) * values
    return jnp.clip(values, min=-most, max=most).astype(held_as)


def setup_inputs(seed: int = 0) -> dict:
    seeds = jax.random.split(jax.random.key(seed), 15)
    receptance = scatter_about(seeds[0], (TOKENS, WIDTH), 1.0, 6.0, ((0, 8), (1, 4)))
    key_in = scatter_about(seeds[1], (TOKENS, WIDTH), 1.0, 6.0, ((0, 8), (1, 4)))
    value_in = scatter_about(seeds[2], (TOKENS, WIDTH), 1.0, 6.0, ((0, 8), (1, 4)))
    decay_in = draw_decay_in(jax.random.fold_in(seeds[14], 71), 0)
    rate_in = draw_rate_in(jax.random.fold_in(seeds[14], 71), 0)
    norm_gain = jnp.clip(1.0 + 0.18 * jax.random.normal(seeds[5], (WIDTH,), jnp.float32), 0.1, 1.9)
    out_weight = scatter_about(seeds[6], (WIDTH, D), WIDTH ** -0.5, 0.125, ((0, 4),))
    moe_in = scatter_about(seeds[7], (MOE_ROWS, D), 1.0, 6.0, ((0, 8),))
    ffn_gain = jnp.clip(1.0 + 0.18 * jax.random.normal(seeds[8], (D,), jnp.float32), 0.1, 1.9)
    routes_keys = jax.random.split(jax.random.fold_in(seeds[9], 1), MOE_ROWS // R_DEV)
    routes_turns = jax.random.permutation(jax.random.fold_in(seeds[9], 3), MOE_ROWS // R_DEV)
    routes = jax.vmap(lambda own, number: routed_block(jax.random.fold_in(seeds[9], 2), own, number, R_DEV, EXPERTS, TOPK, CAP, 1))(routes_keys, routes_turns).reshape((MOE_ROWS, TOPK))
    route_weights = jnp.clip(0.2 + 0.8 * jax.random.uniform(seeds[10], (MOE_ROWS, TOPK), jnp.float32) ** block_levels(seeds[10], (MOE_ROWS, TOPK), ((0, 8),), -0.2, 0.2), 0.2, 1.0)
    gate_weight = scatter_about(seeds[11], (EXPERTS, D, FE), D ** -0.5, 0.09375, ((0, 8), (2, 4)))
    up_weight = scatter_about(seeds[12], (EXPERTS, D, FE), D ** -0.5, 0.09375, ((0, 8), (2, 4)))
    down_weight = scatter_about(seeds[13], (EXPERTS, FE, D), FE ** -0.5, 0.1875, ((0, 8), (2, 4)))
    return {"receptance": receptance, "key_in": key_in, "value_in": value_in, "decay_in": decay_in, "rate_in": rate_in, "norm_gain": norm_gain, "out_weight": out_weight, "moe_in": moe_in, "ffn_gain": ffn_gain, "routes": routes, "route_weights": route_weights, "gate_weight": gate_weight, "up_weight": up_weight, "down_weight": down_weight}


EXACT_MATMUL = lax.Precision.HIGHEST

def mixer_reference(receptance, key_in, value_in, decay_in, rate_in, norm_gain, out_weight):
    shape = (TOKENS, HEADS, HD)
    readout = receptance.astype(jnp.float32).reshape(shape)
    key_rows = key_in.astype(jnp.float32).reshape(shape)
    value_rows = value_in.astype(jnp.float32).reshape(shape)
    log_decay = -jnp.exp(-jax.nn.softplus(-decay_in.astype(jnp.float32)) - 0.5).reshape(shape)
    learn_rate = jax.nn.sigmoid(rate_in.astype(jnp.float32)).reshape(shape)
    unit_key = key_rows / jnp.sqrt(lax.optimization_barrier(jnp.sum(key_rows * key_rows, axis=-1, keepdims=True)) + 1.0)

    def advance(passed_state, inputs):
        current_readout, key_now, value_now, decay_now, rate_now, current_unit_key = inputs
        sequence_walk = jnp.einsum('bw,bwo->bo', current_unit_key, passed_state, precision=EXACT_MATMUL)
        passed_state = jnp.exp(decay_now)[:, :, None] * passed_state - (current_unit_key * rate_now)[:, :, None] * sequence_walk[:, None, :] + (key_now * rate_now)[:, :, None] * value_now[:, None, :]
        return (passed_state, jnp.einsum('bw,bwo->bo', current_readout, passed_state, precision=EXACT_MATMUL))
    start = jnp.zeros((HEADS, HD, HD), jnp.float32)
    _, heads_out = lax.scan(advance, start, (readout, key_rows, value_rows, log_decay, learn_rate, unit_key))
    center = heads_out - lax.optimization_barrier(jnp.mean(heads_out, axis=-1, keepdims=True))
    spread = lax.optimization_barrier(jnp.mean(center * center, axis=-1, keepdims=True))
    normed = center * lax.rsqrt(spread + 1.0) * norm_gain.astype(jnp.float32).reshape(HEADS, HD)
    mixed = normed.reshape(TOKENS, WIDTH).astype(jnp.bfloat16)
    group_width = WIDTH // N_TP

    def add_group(running, group_index):
        columns = lax.dynamic_slice_in_dim(mixed, group_index * group_width, group_width, 1)
        weights = lax.dynamic_slice_in_dim(out_weight, group_index * group_width, group_width, 0)
        product = jnp.dot(columns, weights, preferred_element_type=jnp.float32).astype(jnp.bfloat16)
        product = lax.optimization_barrier(product)
        return (running + product.astype(jnp.float32), None)
    summed, _ = lax.scan(add_group, jnp.zeros((TOKENS, D), jnp.float32), jnp.arange(N_TP, dtype=jnp.int32))
    return summed.astype(jnp.bfloat16)

def expert_reference(moe_in, ffn_gain, routes, route_weights, gate_weight, up_weight, down_weight):
    row_values = moe_in.astype(jnp.float32)
    scaled = row_values * lax.rsqrt(lax.optimization_barrier(jnp.mean(row_values * row_values, axis=-1, keepdims=True)) + 1.0) * ffn_gain
    normed_rows = scaled.astype(jnp.bfloat16)
    pairs = routes.reshape(-1).astype(jnp.int32)
    pair_count = pairs.shape[0]
    onehot = (pairs[:, None] == jnp.arange(EXPERTS, dtype=jnp.int32)[None, :]).astype(jnp.int32)
    slot_rank = lax.optimization_barrier(jnp.sum((jnp.cumsum(onehot, axis=0) - onehot) * onehot, axis=1)).astype(jnp.int32)
    capacity = N_EP * CAP
    position = (pairs * capacity + slot_rank).astype(jnp.int32)
    source = jnp.zeros((EXPERTS * capacity,), jnp.int32).at[position].set(jnp.arange(pair_count, dtype=jnp.int32) // TOPK).reshape(EXPERTS, capacity)
    filled = jnp.zeros((EXPERTS * capacity,), jnp.int32).at[position].set(1).reshape(EXPERTS, capacity)

    def one_expert(operands):
        source_rows, live, gate_matrix, up_matrix, down_matrix = operands
        taken = jnp.where(live[:, None] > 0, normed_rows[source_rows], jnp.zeros((), normed_rows.dtype))
        gate = jnp.dot(taken, gate_matrix, preferred_element_type=jnp.float32)
        up_part = jnp.dot(taken, up_matrix, preferred_element_type=jnp.float32)
        hidden = (jax.nn.silu(gate) * up_part).astype(jnp.bfloat16)
        return jnp.dot(hidden, down_matrix, preferred_element_type=jnp.float32).astype(jnp.bfloat16)
    results = lax.map(one_expert, (source, filled, gate_weight, up_weight, down_weight))
    per_pair = results.reshape(EXPERTS * capacity, D)[position].astype(jnp.float32).reshape(MOE_ROWS, TOPK, D)
    portion = route_weights / lax.optimization_barrier(jnp.sum(route_weights, axis=-1, keepdims=True))
    return lax.optimization_barrier(jnp.sum(portion[:, :, None] * per_pair, axis=1)).astype(jnp.bfloat16)

def reference(receptance, key_in, value_in, decay_in, rate_in, norm_gain, out_weight, moe_in, ffn_gain, routes, route_weights, gate_weight, up_weight, down_weight):
    mixer_out = mixer_reference(receptance, key_in, value_in, decay_in, rate_in, norm_gain, out_weight)
    moe_out = expert_reference(moe_in, ffn_gain, routes, route_weights, gate_weight, up_weight, down_weight)
    return (mixer_out, moe_out)
```

```python
import functools

import jax
import jax.numpy as jnp
from jax import lax
from jax.experimental import pallas as pl
from jax.experimental.pallas import tpu as pltpu
from jax.sharding import PartitionSpec as P

HD = 64
BLOCK = 64
F32 = jnp.float32
BF16 = jnp.bfloat16
MESH = pl.DeviceIdType.MESH


def dot(a, b):
    return jnp.dot(a.astype(BF16), b.astype(BF16), preferred_element_type=F32)


def dot_rows(a, b):
    return lax.dot_general(
        a.astype(BF16), b.astype(BF16), (((1,), (1,)), ((), ())), preferred_element_type=F32
    )


def dot_cols(a, b):
    return lax.dot_general(
        a.astype(BF16), b.astype(BF16), (((0,), (0,)), ((), ())), preferred_element_type=F32
    )


def dot_exact(a, b):
    return jnp.dot(a, b, precision=lax.Precision.HIGHEST, preferred_element_type=F32)


def lane_head(rows, width):
    return lax.broadcasted_iota(jnp.int32, (rows, width), 1) // HD


def spread(packed):
    rows, width = packed.shape
    packed = packed.astype(BF16)
    head = lane_head(rows, width)
    return jnp.concatenate(
        [jnp.where(head == i, packed, jnp.zeros_like(packed)) for i in range(width // HD)], axis=0
    )


def fold(square):
    width = square.shape[1]
    head = lane_head(HD, width)
    out = jnp.zeros((HD, width), F32)
    for i in range(width // HD):
        out = jnp.where(head == i, square[i * HD : (i + 1) * HD], out)
    return out


def head_ones(width):
    row = lax.broadcasted_iota(jnp.int32, (width, width), 0) // HD
    return (row == lane_head(width, width)).astype(F32)


def group_width(columns):
    return HD * max(g for g in (4, 2, 1) if columns % (g * HD) == 0)


def tables_kernel(r_ref, k_ref, v_ref, d_ref, a_ref, read_ref, local_ref, total_ref, carry):
    columns = r_ref.shape[1]
    width = group_width(columns)
    row = lax.broadcasted_iota(jnp.int32, (BLOCK, width), 0)
    lane = lax.broadcasted_iota(jnp.int32, (BLOCK, width), 1) % HD
    strict = lane < row
    closed = lane <= row
    eye = (lane == row).astype(F32)
    tril = (
        lax.broadcasted_iota(jnp.int32, (BLOCK, BLOCK), 1)
        <= lax.broadcasted_iota(jnp.int32, (BLOCK, BLOCK), 0)
    ).astype(F32)
    ones = head_ones(width)

    @pl.when(pl.program_id(0) == 0)
    def _():
        for group in range(columns // width):
            carry[0, group] = eye
            carry[1, group] = jnp.zeros_like(eye)

    for group in range(columns // width):
        at = pl.ds(group * width, width)
        readout = r_ref[:, at].astype(F32)
        key = k_ref[:, at].astype(F32)
        value = v_ref[:, at]
        log_decay = jax.nn.sigmoid(d_ref[:, at].astype(F32)) * -0.6065306597126334
        rate = jax.nn.sigmoid(a_ref[:, at].astype(F32))
        unit = key * lax.rsqrt(dot_exact(key * key, ones) + 1.0)
        inclusive = dot_exact(tril, log_decay)
        total = inclusive[BLOCK - 1 :]
        probe = -unit * jnp.exp(inclusive - log_decay)
        removal = unit * rate
        written = key * rate
        back = jnp.exp(-inclusive)
        tail = jnp.exp(total - inclusive)
        readout = readout * jnp.exp(inclusive)
        left = jnp.concatenate([probe, readout], axis=0)
        on_removal = dot_rows(left, spread(removal * back))
        on_write = dot_rows(left, spread(written * back))
        lower = jnp.where(strict, on_removal[:BLOCK], 0.0)
        reach = jnp.where(closed, on_removal[BLOCK:], 0.0)
        lower_write = jnp.where(strict, on_write[:BLOCK], 0.0)
        reach_write = jnp.where(closed, on_write[BLOCK:], 0.0)
        value_wide = spread(value)
        on_value = dot(jnp.concatenate([lower_write, reach_write], axis=0), value_wide)
        inverse = eye + lower
        power = dot(lower, spread(lower))
        for doubling in range(BLOCK.bit_length() - 2):
            wide = spread(power)
            if doubling < BLOCK.bit_length() - 3:
                both = dot(jnp.concatenate([inverse, power], axis=0), wide)
                inverse = inverse + both[:BLOCK]
                power = both[BLOCK:]
            else:
                inverse = inverse + dot(inverse, wide)
        solved_probe = dot(inverse, spread(probe))
        solved_values = dot(inverse, spread(on_value[:BLOCK]))
        transition = eye * jnp.exp(total) + fold(dot_cols(removal * tail, solved_probe))
        increment = fold(
            dot_cols(
                jnp.concatenate([removal * tail, written * tail], axis=0),
                jnp.concatenate([solved_values.astype(BF16), value], axis=0),
            )
        )
        read_state = readout + dot(reach, spread(solved_probe))
        local_out = dot(reach, spread(solved_values)) + on_value[BLOCK:]
        left = jnp.concatenate([read_state, transition], axis=0)
        on_map = dot(left, spread(carry[0, group]))
        on_add = dot(left, spread(carry[1, group]))
        read_ref[:, at] = on_map[:BLOCK].astype(BF16)
        local_ref[:, at] = on_add[:BLOCK] + local_out
        carry[0, group] = on_map[BLOCK:]
        carry[1, group] = on_add[BLOCK:] + increment
        total_ref[0, group] = on_map[BLOCK:].astype(BF16)
        total_ref[1, group] = (on_add[BLOCK:] + increment).astype(BF16)


def block_tables(receptance, key_in, value_in, decay_in, rate_in):
    tokens, columns = receptance.shape
    width = group_width(columns)
    groups = columns // width
    rows = pl.BlockSpec((BLOCK, columns), lambda b: (b, 0))
    return pl.pallas_call(
        tables_kernel,
        grid=(tokens // BLOCK,),
        in_specs=[rows] * 5,
        out_specs=[rows, rows, pl.BlockSpec((2, groups, HD, width), lambda b: (0, 0, 0, 0))],
        out_shape=[
            jax.ShapeDtypeStruct((tokens, columns), BF16),
            jax.ShapeDtypeStruct((tokens, columns), F32),
            jax.ShapeDtypeStruct((2, groups, HD, width), BF16),
        ],
        scratch_shapes=[pltpu.VMEM((2, groups, HD, width), F32)],
        name="tables",
    )(receptance, key_in, value_in, decay_in, rate_in)


def prefix_kernel(count, own_ref, prior_ref, outgoing, incoming, before, send_sem, recv_sem):
    me = lax.axis_index("ep")
    groups = own_ref.shape[1]
    steps = [1 << s for s in range(count.bit_length() - 1)]
    barrier = pltpu.get_barrier_semaphore()
    for step in steps:

        @pl.when(me + step < count)
        def _():
            pl.semaphore_signal(
                barrier, inc=1, device_id={"ep": me + step}, device_id_type=MESH
            )

        @pl.when(me >= step)
        def _():
            pl.semaphore_signal(
                barrier, inc=1, device_id={"ep": me - step}, device_id_type=MESH
            )

    peers = sum(
        jnp.where(me + step < count, 1, 0) + jnp.where(me >= step, 1, 0) for step in steps
    )
    pl.semaphore_wait(barrier, peers)

    width = own_ref.shape[3]
    lane = lax.broadcasted_iota(jnp.int32, (HD, width), 1) % HD
    eye = (lane == lax.broadcasted_iota(jnp.int32, (HD, width), 0)).astype(F32)
    for group in range(groups):
        before[0, group] = eye
        before[1, group] = jnp.zeros_like(eye)
    for number, step in enumerate(steps):
        last = number == len(steps) - 1
        source = own_ref if number == 0 else outgoing.at[number - 1]
        target = incoming.at[number]
        if last:
            source, target = source.at[1], target.at[1]
        copy = pltpu.make_async_remote_copy(
            src_ref=source,
            dst_ref=target,
            send_sem=send_sem.at[number],
            recv_sem=recv_sem.at[number],
            device_id={"ep": lax.rem(me + step, count)},
            device_id_type=MESH,
        )

        @pl.when(me + step < count)
        def _():
            copy.start()

        @pl.when(me >= step)
        def _():
            copy.wait_recv()
            for group in range(groups):
                left = before[0, group]
                before[1, group] += dot(left, spread(incoming[number, 1, group]))
                if not last:
                    before[0, group] = dot(left, spread(incoming[number, 0, group]))

        if not last:
            for group in range(groups):
                left = own_ref[0, group]
                outgoing[number, 0, group] = dot(left, spread(before[0, group])).astype(BF16)
                outgoing[number, 1, group] = (
                    dot(left, spread(before[1, group])) + own_ref[1, group].astype(F32)
                ).astype(BF16)

        @pl.when(me + step < count)
        def _():
            copy.wait_send()

    prior_ref[...] = before[1].astype(BF16)


def entering(total):
    count = lax.axis_size("ep")
    steps = count.bit_length() - 1
    vmem = pl.BlockSpec(memory_space=pltpu.VMEM)
    return pl.pallas_call(
        functools.partial(prefix_kernel, count),
        out_shape=jax.ShapeDtypeStruct(total.shape[1:], BF16),
        in_specs=[vmem],
        out_specs=vmem,
        scratch_shapes=[
            pltpu.VMEM((steps, *total.shape), BF16),
            pltpu.VMEM((steps, *total.shape), BF16),
            pltpu.VMEM(total.shape, F32),
            pltpu.SemaphoreType.DMA((steps,)),
            pltpu.SemaphoreType.DMA((steps,)),
        ],
        compiler_params=pltpu.CompilerParams(collective_id=0, has_side_effects=True),
        name="prefix",
    )(total)


def project_kernel(read_ref, local_ref, prior_ref, gain_ref, weight_ref, out_ref, mixed):
    groups, _, width = prior_ref.shape

    @pl.when(pl.program_id(0) == 0)
    def _():
        ones = head_ones(width)
        for group in range(groups):
            at = pl.ds(group * width, width)
            heads_out = dot(read_ref[:, at], spread(prior_ref[group])) + local_ref[:, at]
            center = heads_out - dot_exact(heads_out, ones) / HD
            variance = dot_exact(center * center, ones) / HD
            mixed[:, at] = (center * lax.rsqrt(variance + 1.0) * gain_ref[:, at]).astype(BF16)

    out_ref[...] = jnp.dot(
        mixed[...], weight_ref[...], preferred_element_type=F32
    ).astype(BF16)


def project(read, local_out, prior, norm_gain, out_weight):
    tokens, columns = read.shape
    features = out_weight.shape[1]
    tile = features // 4
    whole = pl.BlockSpec((tokens, columns), lambda n: (0, 0))
    return pl.pallas_call(
        project_kernel,
        grid=(features // tile,),
        in_specs=[
            whole,
            whole,
            pl.BlockSpec(prior.shape, lambda n: (0, 0, 0)),
            pl.BlockSpec((1, columns), lambda n: (0, 0)),
            pl.BlockSpec((columns, tile), lambda n: (0, n)),
        ],
        out_specs=pl.BlockSpec((tokens, tile), lambda n: (0, n)),
        out_shape=jax.ShapeDtypeStruct((tokens, features), BF16),
        scratch_shapes=[pltpu.VMEM((tokens, columns), BF16)],
        name="project",
    )(read, local_out, prior, norm_gain[None], out_weight)


def mixer_half(receptance, key_in, value_in, decay_in, rate_in, norm_gain, out_weight):
    read, local_out, total = block_tables(receptance, key_in, value_in, decay_in, rate_in)
    prior = entering(total)
    product = project(read, local_out, prior, norm_gain, out_weight)
    return lax.psum_scatter(product, "tp", scatter_dimension=0, tiled=True)


def hidden_kernel(rows_ref, gate_ref, up_ref, hidden_ref, gate, up):
    step = pl.program_id(0)

    @pl.when(step == 0)
    def _():
        gate[...] = jnp.zeros_like(gate)
        up[...] = jnp.zeros_like(up)

    gate[...] += jnp.dot(rows_ref[0], gate_ref[0], preferred_element_type=F32)
    up[...] += jnp.dot(rows_ref[0], up_ref[0], preferred_element_type=F32)

    @pl.when(step == pl.num_programs(0) - 1)
    def _():
        hidden_ref[...] = (jax.nn.silu(gate[...]) * up[...]).astype(BF16)


def expert_hidden(rows, gate_weight, up_weight):
    parts, row_count, part_width = rows.shape
    units = gate_weight.shape[2]
    weights = pl.BlockSpec((1, part_width, units), lambda t: (0, t, 0))
    return pl.pallas_call(
        hidden_kernel,
        grid=(parts,),
        in_specs=[
            pl.BlockSpec((1, row_count, part_width), lambda t: (t, 0, 0)),
            weights,
            weights,
        ],
        out_specs=pl.BlockSpec((row_count, units), lambda t: (0, 0)),
        out_shape=jax.ShapeDtypeStruct((row_count, units), BF16),
        scratch_shapes=[pltpu.VMEM((row_count, units), F32)] * 2,
        name="hidden",
    )(rows, gate_weight, up_weight)


def expert_half(moe_in, ffn_gain, routes, route_weights, gate_weight, up_weight, down_weight):
    row_count, feature_count = moe_in.shape
    choose_count = routes.shape[1]
    ep_count = lax.axis_size("ep")
    tp_count = lax.axis_size("tp")
    expert_count = gate_weight.shape[0] * ep_count
    capacity = 5 * row_count * choose_count // (4 * expert_count)
    part_width = feature_count // tp_count
    row_values = moe_in.astype(F32)
    scale = lax.rsqrt(jnp.mean(row_values * row_values, axis=-1, keepdims=True) + 1.0)
    first = lax.axis_index("tp") * part_width
    piece = (
        lax.dynamic_slice_in_dim(moe_in, first, part_width, 1).astype(F32)
        * scale
        * lax.dynamic_slice_in_dim(ffn_gain, first, part_width, 0)
    ).astype(BF16)
    portion = route_weights / jnp.sum(route_weights, axis=-1, keepdims=True)
    experts = jnp.arange(expert_count, dtype=jnp.int32)
    table = jnp.sum(
        jnp.where(routes[:, :, None] == experts[None, None, :], portion[:, :, None], 0.0), axis=1
    )
    high = table.astype(BF16)
    low = (table - high.astype(F32)).astype(BF16)
    extra = jnp.pad(jnp.concatenate([high, low], axis=1), ((0, 0), (0, 128 - 2 * expert_count)))
    arrived = lax.all_gather(jnp.concatenate([piece, extra], axis=1), "ep")
    mine = lax.axis_index("ep")
    shares = arrived[:, :, part_width:].astype(F32)
    shares = jnp.sum(
        jnp.where(
            lax.broadcasted_iota(jnp.int32, (1, 1, 128), 2) % expert_count == mine, shares, 0.0
        )
        * (lax.broadcasted_iota(jnp.int32, (1, 1, 128), 2) < 2 * expert_count),
        axis=-1,
    )
    named = shares > 0
    earlier = jnp.triu(jnp.ones((row_count, row_count), F32), 1)
    rank = jnp.dot(named.astype(F32), earlier)
    slots = jnp.arange(capacity, dtype=F32)
    chosen = (rank[:, None, :] == slots[None, :, None]) & named[:, None, :]
    onehot = chosen.astype(BF16)
    rows = jnp.einsum(
        "scr,srn->scn", onehot, arrived[:, :, :part_width], preferred_element_type=F32
    ).astype(BF16)
    rows = lax.all_gather(rows.reshape(ep_count * capacity, part_width), "tp")
    hidden = expert_hidden(rows, gate_weight, up_weight)
    hidden = lax.all_gather(hidden, "tp", axis=1, tiled=True)
    result = jnp.dot(hidden, down_weight[0], preferred_element_type=F32)
    slot_share = jnp.sum(jnp.where(chosen, shares[:, None, :], 0.0), axis=-1)
    result = result.reshape(ep_count, capacity, -1) * slot_share[:, :, None]
    placed = jnp.einsum(
        "scr,scd->srd", onehot, result.astype(BF16), preferred_element_type=F32
    ).astype(BF16)
    return lax.psum_scatter(
        placed.reshape(ep_count * row_count, -1), "ep", scatter_dimension=0, tiled=True
    )


def local(
    receptance,
    key_in,
    value_in,
    decay_in,
    rate_in,
    norm_gain,
    out_weight,
    moe_in,
    ffn_gain,
    routes,
    route_weights,
    gate_weight,
    up_weight,
    down_weight,
):
    mixer_out = mixer_half(receptance, key_in, value_in, decay_in, rate_in, norm_gain, out_weight)
    moe_out = expert_half(
        moe_in, ffn_gain, routes, route_weights, gate_weight, up_weight, down_weight
    )
    return (mixer_out, moe_out)


def solution(mesh):
    return jax.shard_map(
        local,
        mesh=mesh,
        in_specs=(
            P("ep", "tp"),
            P("ep", "tp"),
            P("ep", "tp"),
            P("ep", "tp"),
            P("ep", "tp"),
            P("tp"),
            P("tp", None),
            P("ep", None),
            P(),
            P("ep", None),
            P("ep", None),
            P("ep", None, "tp"),
            P("ep", None, "tp"),
            P("ep", None, "tp"),
        ),
        out_specs=(P(("ep", "tp"), None), P("ep", "tp")),
        check_vma=False,
    )
```

```python
import functools

import jax
import jax.numpy as jnp
from jax import lax
from jax.experimental import pallas as pl
from jax.experimental.pallas import tpu as pltpu
from jax.sharding import PartitionSpec as P

HD = 64
BLOCK = 64
F32 = jnp.float32
BF16 = jnp.bfloat16
MESH = pl.DeviceIdType.MESH


def dot(a, b):
    return jnp.dot(a.astype(BF16), b.astype(BF16), preferred_element_type=F32)


def dot_rows(a, b):
    return lax.dot_general(
        a.astype(BF16), b.astype(BF16), (((1,), (1,)), ((), ())), preferred_element_type=F32
    )


def dot_cols(a, b):
    return lax.dot_general(
        a.astype(BF16), b.astype(BF16), (((0,), (0,)), ((), ())), preferred_element_type=F32
    )


def dot_exact(a, b):
    return jnp.dot(a, b, precision=lax.Precision.HIGHEST, preferred_element_type=F32)


def lane_head(rows, width):
    return lax.broadcasted_iota(jnp.int32, (rows, width), 1) // HD


def spread(packed):
    rows, width = packed.shape
    packed = packed.astype(BF16)
    head = lane_head(rows, width)
    return jnp.concatenate(
        [jnp.where(head == i, packed, jnp.zeros_like(packed)) for i in range(width // HD)], axis=0
    )


def fold(square):
    width = square.shape[1]
    head = lane_head(HD, width)
    out = jnp.zeros((HD, width), F32)
    for i in range(width // HD):
        out = jnp.where(head == i, square[i * HD : (i + 1) * HD], out)
    return out


def head_ones(width):
    row = lax.broadcasted_iota(jnp.int32, (width, width), 0) // HD
    return (row == lane_head(width, width)).astype(F32)


def group_width(columns):
    return HD * max(g for g in (4, 2, 1) if columns % (g * HD) == 0)


def tables_kernel(r_ref, k_ref, v_ref, d_ref, a_ref, read_ref, local_ref, total_ref, carry):
    columns = r_ref.shape[1]
    width = group_width(columns)
    row = lax.broadcasted_iota(jnp.int32, (BLOCK, width), 0)
    lane = lax.broadcasted_iota(jnp.int32, (BLOCK, width), 1) % HD
    strict = lane < row
    closed = lane <= row
    eye = (lane == row).astype(F32)
    tril = (
        lax.broadcasted_iota(jnp.int32, (BLOCK, BLOCK), 1)
        <= lax.broadcasted_iota(jnp.int32, (BLOCK, BLOCK), 0)
    ).astype(F32)
    ones = head_ones(width)

    @pl.when(pl.program_id(0) == 0)
    def _():
        for group in range(columns // width):
            carry[0, group] = eye
            carry[1, group] = jnp.zeros_like(eye)

    for group in range(columns // width):
        at = pl.ds(group * width, width)
        readout = r_ref[:, at].astype(F32)
        key = k_ref[:, at].astype(F32)
        value = v_ref[:, at]
        log_decay = jax.nn.sigmoid(d_ref[:, at].astype(F32)) * -0.6065306597126334
        rate = jax.nn.sigmoid(a_ref[:, at].astype(F32))
        unit = key * lax.rsqrt(dot_exact(key * key, ones) + 1.0)
        inclusive = dot_exact(tril, log_decay)
        total = inclusive[BLOCK - 1 :]
        probe = -unit * jnp.exp(inclusive - log_decay)
        removal = unit * rate
        written = key * rate
        back = jnp.exp(-inclusive)
        tail = jnp.exp(total - inclusive)
        readout = readout * jnp.exp(inclusive)
        left = jnp.concatenate([probe, readout], axis=0)
        on_removal = dot_rows(left, spread(removal * back))
        on_write = dot_rows(left, spread(written * back))
        lower = jnp.where(strict, on_removal[:BLOCK], 0.0)
        reach = jnp.where(closed, on_removal[BLOCK:], 0.0)
        lower_write = jnp.where(strict, on_write[:BLOCK], 0.0)
        reach_write = jnp.where(closed, on_write[BLOCK:], 0.0)
        value_wide = spread(value)
        on_value = dot(jnp.concatenate([lower_write, reach_write], axis=0), value_wide)
        inverse = eye + lower
        power = dot(lower, spread(lower))
        for doubling in range(BLOCK.bit_length() - 2):
            wide = spread(power)
            if doubling < BLOCK.bit_length() - 3:
                both = dot(jnp.concatenate([inverse, power], axis=0), wide)
                inverse = inverse + both[:BLOCK]
                power = both[BLOCK:]
            else:
                inverse = inverse + dot(inverse, wide)
        solved_probe = dot(inverse, spread(probe))
        solved_values = dot(inverse, spread(on_value[:BLOCK]))
        transition = eye * jnp.exp(total) + fold(dot_cols(removal * tail, solved_probe))
        increment = fold(
            dot_cols(
                jnp.concatenate([removal * tail, written * tail], axis=0),
                jnp.concatenate([solved_values.astype(BF16), value], axis=0),
            )
        )
        read_state = readout + dot(reach, spread(solved_probe))
        local_out = dot(reach, spread(solved_values)) + on_value[BLOCK:]
        left = jnp.concatenate([read_state, transition], axis=0)
        on_map = dot(left, spread(carry[0, group]))
        on_add = dot(left, spread(carry[1, group]))
        read_ref[:, at] = on_map[:BLOCK].astype(BF16)
        local_ref[:, at] = on_add[:BLOCK] + local_out
        carry[0, group] = on_map[BLOCK:]
        carry[1, group] = on_add[BLOCK:] + increment
        total_ref[0, group] = on_map[BLOCK:].astype(BF16)
        total_ref[1, group] = (on_add[BLOCK:] + increment).astype(BF16)


def block_tables(receptance, key_in, value_in, decay_in, rate_in):
    tokens, columns = receptance.shape
    width = group_width(columns)
    groups = columns // width
    rows = pl.BlockSpec((BLOCK, columns), lambda b: (b, 0))
    return pl.pallas_call(
        tables_kernel,
        grid=(tokens // BLOCK,),
        in_specs=[rows] * 5,
        out_specs=[rows, rows, pl.BlockSpec((2, groups, HD, width), lambda b: (0, 0, 0, 0))],
        out_shape=[
            jax.ShapeDtypeStruct((tokens, columns), BF16),
            jax.ShapeDtypeStruct((tokens, columns), F32),
            jax.ShapeDtypeStruct((2, groups, HD, width), BF16),
        ],
        scratch_shapes=[pltpu.VMEM((2, groups, HD, width), F32)],
        name="tables",
    )(receptance, key_in, value_in, decay_in, rate_in)


def prefix_kernel(count, own_ref, prior_ref, outgoing, incoming, before, send_sem, recv_sem):
    me = lax.axis_index("ep")
    groups = own_ref.shape[1]
    steps = [1 << s for s in range(count.bit_length() - 1)]
    barrier = pltpu.get_barrier_semaphore()
    for step in steps:

        @pl.when(me + step < count)
        def _():
            pl.semaphore_signal(
                barrier, inc=1, device_id={"ep": me + step}, device_id_type=MESH
            )

        @pl.when(me >= step)
        def _():
            pl.semaphore_signal(
                barrier, inc=1, device_id={"ep": me - step}, device_id_type=MESH
            )

    peers = sum(
        jnp.where(me + step < count, 1, 0) + jnp.where(me >= step, 1, 0) for step in steps
    )
    pl.semaphore_wait(barrier, peers)

    width = own_ref.shape[3]
    lane = lax.broadcasted_iota(jnp.int32, (HD, width), 1) % HD
    eye = (lane == lax.broadcasted_iota(jnp.int32, (HD, width), 0)).astype(F32)
    for group in range(groups):
        before[0, group] = eye
        before[1, group] = jnp.zeros_like(eye)
    for number, step in enumerate(steps):
        last = number == len(steps) - 1
        source = own_ref if number == 0 else outgoing.at[number - 1]
        target = incoming.at[number]
        if last:
            source, target = source.at[1], target.at[1]
        copy = pltpu.make_async_remote_copy(
            src_ref=source,
            dst_ref=target,
            send_sem=send_sem.at[number],
            recv_sem=recv_sem.at[number],
            device_id={"ep": lax.rem(me + step, count)},
            device_id_type=MESH,
        )

        @pl.when(me + step < count)
        def _():
            copy.start()

        @pl.when(me >= step)
        def _():
            copy.wait_recv()
            for group in range(groups):
                left = before[0, group]
                before[1, group] += dot(left, spread(incoming[number, 1, group]))
                if not last:
                    before[0, group] = dot(left, spread(incoming[number, 0, group]))

        if not last:
            for group in range(groups):
                left = own_ref[0, group]
                outgoing[number, 0, group] = dot(left, spread(before[0, group])).astype(BF16)
                outgoing[number, 1, group] = (
                    dot(left, spread(before[1, group])) + own_ref[1, group].astype(F32)
                ).astype(BF16)

        @pl.when(me + step < count)
        def _():
            copy.wait_send()

    prior_ref[...] = before[1].astype(BF16)


def entering(total):
    count = lax.axis_size("ep")
    steps = count.bit_length() - 1
    vmem = pl.BlockSpec(memory_space=pltpu.VMEM)
    return pl.pallas_call(
        functools.partial(prefix_kernel, count),
        out_shape=jax.ShapeDtypeStruct(total.shape[1:], BF16),
        in_specs=[vmem],
        out_specs=vmem,
        scratch_shapes=[
            pltpu.VMEM((steps, *total.shape), BF16),
            pltpu.VMEM((steps, *total.shape), BF16),
            pltpu.VMEM(total.shape, F32),
            pltpu.SemaphoreType.DMA((steps,)),
            pltpu.SemaphoreType.DMA((steps,)),
        ],
        compiler_params=pltpu.CompilerParams(collective_id=0, has_side_effects=True),
        name="prefix",
    )(total)


def project_kernel(read_ref, local_ref, prior_ref, gain_ref, weight_ref, out_ref, mixed):
    groups, _, width = prior_ref.shape

    @pl.when(pl.program_id(0) == 0)
    def _():
        ones = head_ones(width)
        for group in range(groups):
            at = pl.ds(group * width, width)
            heads_out = dot(read_ref[:, at], spread(prior_ref[group])) + local_ref[:, at]
            center = heads_out - dot_exact(heads_out, ones) / HD
            variance = dot_exact(center * center, ones) / HD
            mixed[:, at] = (center * lax.rsqrt(variance + 1.0) * gain_ref[:, at]).astype(BF16)

    out_ref[...] = jnp.dot(
        mixed[...], weight_ref[...], preferred_element_type=F32
    ).astype(BF16)


def project(read, local_out, prior, norm_gain, out_weight):
    tokens, columns = read.shape
    features = out_weight.shape[1]
    tile = features // 4
    whole = pl.BlockSpec((tokens, columns), lambda n: (0, 0))
    return pl.pallas_call(
        project_kernel,
        grid=(features // tile,),
        in_specs=[
            whole,
            whole,
            pl.BlockSpec(prior.shape, lambda n: (0, 0, 0)),
            pl.BlockSpec((1, columns), lambda n: (0, 0)),
            pl.BlockSpec((columns, tile), lambda n: (0, n)),
        ],
        out_specs=pl.BlockSpec((tokens, tile), lambda n: (0, n)),
        out_shape=jax.ShapeDtypeStruct((tokens, features), BF16),
        scratch_shapes=[pltpu.VMEM((tokens, columns), BF16)],
        name="project",
    )(read, local_out, prior, norm_gain[None], out_weight)


def scatter(product):
    return lax.psum_scatter(product, "tp", scatter_dimension=0, tiled=True)


def hidden_kernel(rows_ref, gate_ref, up_ref, hidden_ref, gate, up):
    step = pl.program_id(0)

    @pl.when(step == 0)
    def _():
        gate[...] = jnp.zeros_like(gate)
        up[...] = jnp.zeros_like(up)

    gate[...] += jnp.dot(rows_ref[0], gate_ref[0], preferred_element_type=F32)
    up[...] += jnp.dot(rows_ref[0], up_ref[0], preferred_element_type=F32)

    @pl.when(step == pl.num_programs(0) - 1)
    def _():
        hidden_ref[...] = (jax.nn.silu(gate[...]) * up[...]).astype(BF16)


def expert_hidden(rows, gate_weight, up_weight):
    parts, row_count, part_width = rows.shape
    units = gate_weight.shape[2]
    weights = pl.BlockSpec((1, part_width, units), lambda t: (0, t, 0))
    return pl.pallas_call(
        hidden_kernel,
        grid=(parts,),
        in_specs=[
            pl.BlockSpec((1, row_count, part_width), lambda t: (t, 0, 0)),
            weights,
            weights,
        ],
        out_specs=pl.BlockSpec((row_count, units), lambda t: (0, 0)),
        out_shape=jax.ShapeDtypeStruct((row_count, units), BF16),
        scratch_shapes=[pltpu.VMEM((row_count, units), F32)] * 2,
        name="hidden",
    )(rows, gate_weight, up_weight)


def return_kernel(count, placed_ref, out_ref, pair_in, held, from_left, from_right, sems):
    me = lax.axis_index("ep")
    chips = count // 2
    core = lax.rem(me, 2)
    chip = me // 2
    partner = me + 1 - 2 * core
    barrier = pltpu.get_barrier_semaphore()

    def signal(to):
        pl.semaphore_signal(barrier, inc=1, device_id={"ep": to}, device_id_type=MESH)

    signal(partner)
    pl.when(chip > 0)(lambda: signal(me - 2))
    pl.when(chip < chips - 1)(lambda: signal(me + 2))
    pl.semaphore_wait(
        barrier, 1 + jnp.where(chip > 0, 1, 0) + jnp.where(chip < chips - 1, 1, 0)
    )

    def send(source, target, kind, slot, to):
        return pltpu.make_async_remote_copy(
            src_ref=source,
            dst_ref=target,
            send_sem=sems.at[kind, 0, slot],
            recv_sem=sems.at[kind, 1, slot],
            device_id={"ep": to},
            device_id_type=MESH,
        )

    order = []
    for step in range(chips):
        order += [at for at in (chips - 1 - step, step) if at not in order]
    pairs = [
        send(placed_ref.at[2 * at + 1 - core], pair_in.at[at], 0, at, partner)
        for at in range(chips)
    ]
    rights = [
        send(from_left.at[at], from_left.at[at], 1, at, jnp.minimum(me + 2, count - 2 + core))
        for at in range(chips)
    ]
    lefts = [
        send(from_right.at[at], from_right.at[at], 2, at, jnp.maximum(me - 2, core))
        for at in range(chips)
    ]
    first_rights = [
        send(held.at[at], from_left.at[at], 1, at, jnp.minimum(me + 2, count - 2 + core))
        for at in range(chips)
    ]
    first_lefts = [
        send(held.at[at], from_right.at[at], 2, at, jnp.maximum(me - 2, core))
        for at in range(chips)
    ]
    for at in order:
        pairs[at].start()

    def pair_sum(at):
        pairs[at].wait_recv()
        held[at] = (
            placed_ref[2 * at + core].astype(F32) + pair_in[at].astype(F32)
        ).astype(BF16)

    def forward(at, moving, first, relay, landing, origin):
        @pl.when(moving & origin)
        def _():
            first.start()

        @pl.when(moving & jnp.logical_not(origin))
        def _():
            relay.wait_recv()
            landing[at] = (landing[at].astype(F32) + held[at].astype(F32)).astype(BF16)
            relay.start()

    ready = []
    for step in range(chips):
        for at in (chips - 1 - step, step):
            if at not in ready:
                pair_sum(at)
                ready.append(at)
        at = chips - 1 - step
        if at > 0:
            forward(at, at > chip, first_rights[at], rights[at], from_left, chip == 0)
        at = step
        if at < chips - 1:
            forward(at, at < chip, first_lefts[at], lefts[at], from_right, chip == chips - 1)
    out_ref[...] = held[chip]

    for at in range(chips):

        @pl.when((at == chip) & (chip > 0))
        def _():
            rights[at].wait_recv()
            out_ref[...] = (out_ref[...].astype(F32) + from_left[at].astype(F32)).astype(BF16)

        @pl.when((at == chip) & (chip < chips - 1))
        def _():
            lefts[at].wait_recv()
            out_ref[...] = (out_ref[...].astype(F32) + from_right[at].astype(F32)).astype(BF16)

    for at in range(chips):
        pairs[at].wait_send()
        pl.when(at > chip)(rights[at].wait_send)
        pl.when(at < chip)(lefts[at].wait_send)


def returned(placed):
    count, rows, width = placed.shape
    chips = count // 2
    vmem = pl.BlockSpec(memory_space=pltpu.VMEM)
    return pl.pallas_call(
        functools.partial(return_kernel, count),
        out_shape=jax.ShapeDtypeStruct((rows, width), BF16),
        in_specs=[vmem],
        out_specs=vmem,
        scratch_shapes=[pltpu.VMEM((chips, rows, width), BF16)] * 4
        + [pltpu.SemaphoreType.DMA((3, 2, chips))],
        compiler_params=pltpu.CompilerParams(collective_id=1, has_side_effects=True),
        name="return",
    )(placed)


def both_halves(
    mixer_args,
    norm_gain,
    out_weight,
    moe_in,
    ffn_gain,
    routes,
    route_weights,
    gate_weight,
    up_weight,
    down_weight,
):
    row_count, feature_count = moe_in.shape
    choose_count = routes.shape[1]
    ep_count = lax.axis_size("ep")
    tp_count = lax.axis_size("tp")
    expert_count = gate_weight.shape[0] * ep_count
    capacity = 5 * row_count * choose_count // (4 * expert_count)
    part_width = feature_count // tp_count
    row_values = moe_in.astype(F32)
    scale = lax.rsqrt(jnp.mean(row_values * row_values, axis=-1, keepdims=True) + 1.0)
    first = lax.axis_index("tp") * part_width
    piece = (
        lax.dynamic_slice_in_dim(moe_in, first, part_width, 1).astype(F32)
        * scale
        * lax.dynamic_slice_in_dim(ffn_gain, first, part_width, 0)
    ).astype(BF16)
    portion = route_weights / jnp.sum(route_weights, axis=-1, keepdims=True)
    experts = jnp.arange(expert_count, dtype=jnp.int32)
    table = jnp.sum(
        jnp.where(routes[:, :, None] == experts[None, None, :], portion[:, :, None], 0.0), axis=1
    )
    high = table.astype(BF16)
    low = (table - high.astype(F32)).astype(BF16)
    extra = jnp.pad(jnp.concatenate([high, low], axis=1), ((0, 0), (0, 128 - 2 * expert_count)))
    arrived = lax.all_gather(jnp.concatenate([piece, extra], axis=1), "ep")
    tables = block_tables(*mixer_args)
    arrived, (read, local_out, total) = lax.optimization_barrier((arrived, tables))
    mine = lax.axis_index("ep")
    shares = arrived[:, :, part_width:].astype(F32)
    shares = jnp.sum(
        jnp.where(
            lax.broadcasted_iota(jnp.int32, (1, 1, 128), 2) % expert_count == mine, shares, 0.0
        )
        * (lax.broadcasted_iota(jnp.int32, (1, 1, 128), 2) < 2 * expert_count),
        axis=-1,
    )
    named = shares > 0
    earlier = jnp.triu(jnp.ones((row_count, row_count), F32), 1)
    rank = jnp.dot(named.astype(F32), earlier)
    slots = jnp.arange(capacity, dtype=F32)
    chosen = (rank[:, None, :] == slots[None, :, None]) & named[:, None, :]
    onehot = chosen.astype(BF16)
    rows = jnp.einsum(
        "scr,srn->scn", onehot, arrived[:, :, :part_width], preferred_element_type=F32
    ).astype(BF16)
    rows = lax.all_gather(rows.reshape(ep_count * capacity, part_width), "tp")
    prior = entering(total)
    product = project(read, local_out, prior, norm_gain, out_weight)
    rows, product = lax.optimization_barrier((rows, product))
    hidden = expert_hidden(rows, gate_weight, up_weight)
    hidden = lax.all_gather(hidden, "tp", axis=1, tiled=True)
    hidden, product = lax.optimization_barrier((hidden, product))
    result = jnp.dot(hidden, down_weight[0], preferred_element_type=F32)
    slot_share = jnp.sum(jnp.where(chosen, shares[:, None, :], 0.0), axis=-1)
    result = result.reshape(ep_count, capacity, -1) * slot_share[:, :, None]
    placed = jnp.einsum(
        "scr,scd->srd", onehot, result.astype(BF16), preferred_element_type=F32
    ).astype(BF16)
    return scatter(product), returned(placed)


def local(
    receptance,
    key_in,
    value_in,
    decay_in,
    rate_in,
    norm_gain,
    out_weight,
    moe_in,
    ffn_gain,
    routes,
    route_weights,
    gate_weight,
    up_weight,
    down_weight,
):
    return both_halves(
        (receptance, key_in, value_in, decay_in, rate_in),
        norm_gain,
        out_weight,
        moe_in,
        ffn_gain,
        routes,
        route_weights,
        gate_weight,
        up_weight,
        down_weight,
    )


def solution(mesh):
    return jax.shard_map(
        local,
        mesh=mesh,
        in_specs=(
            P("ep", "tp"),
            P("ep", "tp"),
            P("ep", "tp"),
            P("ep", "tp"),
            P("ep", "tp"),
            P("tp"),
            P("tp", None),
            P("ep", None),
            P(),
            P("ep", None),
            P("ep", None),
            P("ep", None, "tp"),
            P("ep", None, "tp"),
            P("ep", None, "tp"),
        ),
        out_specs=(P(("ep", "tp"), None), P("ep", "tp")),
        check_vma=False,
    )
```

```python
import functools

import jax
import jax.numpy as jnp
from jax import lax
from jax.experimental import pallas as pl
from jax.experimental.pallas import tpu as pltpu
from jax.sharding import PartitionSpec as P

HD = 64
BLOCK = 64
F32 = jnp.float32
BF16 = jnp.bfloat16
MESH = pl.DeviceIdType.MESH


def dot(a, b):
    return jnp.dot(a.astype(BF16), b.astype(BF16), preferred_element_type=F32)


def dot_rows(a, b):
    return lax.dot_general(
        a.astype(BF16), b.astype(BF16), (((1,), (1,)), ((), ())), preferred_element_type=F32
    )


def dot_cols(a, b):
    return lax.dot_general(
        a.astype(BF16), b.astype(BF16), (((0,), (0,)), ((), ())), preferred_element_type=F32
    )


def dot_exact(a, b):
    return jnp.dot(a, b, precision=lax.Precision.HIGHEST, preferred_element_type=F32)


def lane_head(rows, width):
    return lax.broadcasted_iota(jnp.int32, (rows, width), 1) // HD


def spread(packed):
    rows, width = packed.shape
    packed = packed.astype(BF16)
    head = lane_head(rows, width)
    return jnp.concatenate(
        [jnp.where(head == i, packed, jnp.zeros_like(packed)) for i in range(width // HD)], axis=0
    )


def fold(square):
    width = square.shape[1]
    head = lane_head(HD, width)
    out = jnp.zeros((HD, width), F32)
    for i in range(width // HD):
        out = jnp.where(head == i, square[i * HD : (i + 1) * HD], out)
    return out


def head_ones(width):
    row = lax.broadcasted_iota(jnp.int32, (width, width), 0) // HD
    return (row == lane_head(width, width)).astype(F32)


def group_width(columns):
    return HD * max(g for g in (4, 2, 1) if columns % (g * HD) == 0)


def tables_kernel(r_ref, k_ref, v_ref, d_ref, a_ref, read_ref, local_ref, total_ref, carry):
    columns = r_ref.shape[1]
    width = group_width(columns)
    row = lax.broadcasted_iota(jnp.int32, (BLOCK, width), 0)
    lane = lax.broadcasted_iota(jnp.int32, (BLOCK, width), 1) % HD
    strict = lane < row
    closed = lane <= row
    eye = (lane == row).astype(F32)
    tril = (
        lax.broadcasted_iota(jnp.int32, (BLOCK, BLOCK), 1)
        <= lax.broadcasted_iota(jnp.int32, (BLOCK, BLOCK), 0)
    ).astype(F32)
    ones = head_ones(width)

    @pl.when(pl.program_id(0) == 0)
    def _():
        for group in range(columns // width):
            carry[0, group] = eye
            carry[1, group] = jnp.zeros_like(eye)

    for group in range(columns // width):
        at = pl.ds(group * width, width)
        readout = r_ref[:, at].astype(F32)
        key = k_ref[:, at].astype(F32)
        value = v_ref[:, at]
        log_decay = jax.nn.sigmoid(d_ref[:, at].astype(F32)) * -0.6065306597126334
        rate = jax.nn.sigmoid(a_ref[:, at].astype(F32))
        unit = key * lax.rsqrt(dot_exact(key * key, ones) + 1.0)
        inclusive = dot_exact(tril, log_decay)
        total = inclusive[BLOCK - 1 :]
        probe = -unit * jnp.exp(inclusive - log_decay)
        removal = unit * rate
        written = key * rate
        back = jnp.exp(-inclusive)
        tail = jnp.exp(total - inclusive)
        readout = readout * jnp.exp(inclusive)
        left = jnp.concatenate([probe, readout], axis=0)
        on_removal = dot_rows(left, spread(removal * back))
        on_write = dot_rows(left, spread(written * back))
        lower = jnp.where(strict, on_removal[:BLOCK], 0.0)
        reach = jnp.where(closed, on_removal[BLOCK:], 0.0)
        lower_write = jnp.where(strict, on_write[:BLOCK], 0.0)
        reach_write = jnp.where(closed, on_write[BLOCK:], 0.0)
        value_wide = spread(value)
        on_value = dot(jnp.concatenate([lower_write, reach_write], axis=0), value_wide)
        inverse = eye + lower
        power = dot(lower, spread(lower))
        for doubling in range(BLOCK.bit_length() - 2):
            wide = spread(power)
            if doubling < BLOCK.bit_length() - 3:
                both = dot(jnp.concatenate([inverse, power], axis=0), wide)
                inverse = inverse + both[:BLOCK]
                power = both[BLOCK:]
            else:
                inverse = inverse + dot(inverse, wide)
        solved_probe = dot(inverse, spread(probe))
        solved_values = dot(inverse, spread(on_value[:BLOCK]))
        transition = eye * jnp.exp(total) + fold(dot_cols(removal * tail, solved_probe))
        increment = fold(
            dot_cols(
                jnp.concatenate([removal * tail, written * tail], axis=0),
                jnp.concatenate([solved_values.astype(BF16), value], axis=0),
            )
        )
        read_state = readout + dot(reach, spread(solved_probe))
        local_out = dot(reach, spread(solved_values)) + on_value[BLOCK:]
        left = jnp.concatenate([read_state, transition], axis=0)
        on_map = dot(left, spread(carry[0, group]))
        on_add = dot(left, spread(carry[1, group]))
        read_ref[:, at] = on_map[:BLOCK].astype(BF16)
        local_ref[:, at] = on_add[:BLOCK] + local_out
        carry[0, group] = on_map[BLOCK:]
        carry[1, group] = on_add[BLOCK:] + increment
        total_ref[0, group] = on_map[BLOCK:].astype(BF16)
        total_ref[1, group] = (on_add[BLOCK:] + increment).astype(BF16)


def block_tables(receptance, key_in, value_in, decay_in, rate_in):
    tokens, columns = receptance.shape
    width = group_width(columns)
    groups = columns // width
    rows = pl.BlockSpec((BLOCK, columns), lambda b: (b, 0))
    return pl.pallas_call(
        tables_kernel,
        grid=(tokens // BLOCK,),
        in_specs=[rows] * 5,
        out_specs=[rows, rows, pl.BlockSpec((2, groups, HD, width), lambda b: (0, 0, 0, 0))],
        out_shape=[
            jax.ShapeDtypeStruct((tokens, columns), BF16),
            jax.ShapeDtypeStruct((tokens, columns), F32),
            jax.ShapeDtypeStruct((2, groups, HD, width), BF16),
        ],
        scratch_shapes=[pltpu.VMEM((2, groups, HD, width), F32)],
        name="tables",
    )(receptance, key_in, value_in, decay_in, rate_in)


def flip(me, bits):
    bit = 1
    while bit <= bits:
        if bits & bit:
            me = me + bit - 2 * bit * ((me // bit) % 2)
        bit *= 2
    return me


class Exchange:
    def __init__(self, count, own, slots, sems):
        me = lax.axis_index("tp")
        half = own.shape[0] // 2
        bits = [1 << b for b in range(count.bit_length() - 1)]
        self.count, self.copies, self.heads, self.relays, self.seen = count, {}, [], [], set()
        for number in range(len(bits)):
            for stream, order in enumerate((bits, bits[::-1])):
                at = pl.ds(stream * half, half)
                known = [0]
                for bit in order[:number]:
                    known += [k ^ bit for k in known]
                for from_delta in known:
                    bit = order[number]
                    key = (stream, from_delta ^ bit)
                    owner = flip(me, from_delta)
                    self.copies[key] = pltpu.make_async_remote_copy(
                        src_ref=slots.at[owner, at] if from_delta else own.at[at],
                        dst_ref=slots.at[owner, at],
                        send_sem=sems.at[0, stream, key[1]],
                        recv_sem=sems.at[1, stream, key[1]],
                        device_id={"tp": flip(me, bit)},
                        device_id_type=MESH,
                    )
                    if from_delta:
                        self.relays.append((key, from_delta))
                    else:
                        self.heads.append(key)

    def start(self):
        for key in self.heads:
            self.copies[key].start()

    def arrive(self, stream, delta):
        if (stream, delta) not in self.seen:
            self.seen.add((stream, delta))
            self.copies[stream, delta].wait_recv()

    def relay(self):
        for key, from_delta in self.relays:
            self.arrive(key[0], from_delta)
            self.copies[key].start()

    def wait(self, delta):
        for stream in (0, 1):
            self.arrive(stream, delta)

    def finish(self):
        for copy in self.copies.values():
            copy.wait_send()


def prefix(count, own_ref, outgoing, incoming, before, send_sem, recv_sem):
    me = lax.axis_index("ep")
    groups = own_ref.shape[1]
    steps = [1 << s for s in range(count.bit_length() - 1)]
    width = own_ref.shape[3]
    lane = lax.broadcasted_iota(jnp.int32, (HD, width), 1) % HD
    eye = (lane == lax.broadcasted_iota(jnp.int32, (HD, width), 0)).astype(F32)
    for group in range(groups):
        before[0, group] = eye
        before[1, group] = jnp.zeros_like(eye)
    for number, step in enumerate(steps):
        last = number == len(steps) - 1
        source = own_ref if number == 0 else outgoing.at[number - 1]
        target = incoming.at[number]
        if last:
            source, target = source.at[1], target.at[1]
        copy = pltpu.make_async_remote_copy(
            src_ref=source,
            dst_ref=target,
            send_sem=send_sem.at[number],
            recv_sem=recv_sem.at[number],
            device_id={"ep": lax.rem(me + step, count)},
            device_id_type=MESH,
        )

        @pl.when(me + step < count)
        def _():
            copy.start()

        @pl.when(me >= step)
        def _():
            copy.wait_recv()
            for group in range(groups):
                left = before[0, group]
                before[1, group] += dot(left, spread(incoming[number, 1, group]))
                if not last:
                    before[0, group] = dot(left, spread(incoming[number, 0, group]))

        if not last:
            for group in range(groups):
                left = own_ref[0, group]
                outgoing[number, 0, group] = dot(left, spread(before[0, group])).astype(BF16)
                outgoing[number, 1, group] = (
                    dot(left, spread(before[1, group])) + own_ref[1, group].astype(F32)
                ).astype(BF16)

        @pl.when(me + step < count)
        def _():
            copy.wait_send()


def experts_kernel(
    tp_count,
    ep_count,
    rows_ref,
    gate_hbm,
    up_hbm,
    down_hbm,
    share_ref,
    total_ref,
    read_ref,
    local_ref,
    gain_ref,
    weight_hbm,
    product_ref,
    result_ref,
    slots,
    hidden_slots,
    hidden,
    gate_w,
    up_w,
    down_w,
    out_w,
    gate,
    up,
    down,
    mixed,
    outgoing,
    incoming,
    before,
    send_sem,
    recv_sem,
    row_sems,
    hidden_sems,
    load_sems,
):
    me = lax.axis_index("tp")
    place = lax.axis_index("ep")
    steps = [1 << s for s in range(ep_count.bit_length() - 1)]
    bits = [1 << b for b in range(tp_count.bit_length() - 1)]
    loads = [
        pltpu.make_async_copy(source, target, load_sems.at[i])
        for i, (source, target) in enumerate(
            ((gate_hbm, gate_w), (up_hbm, up_w), (down_hbm, down_w), (weight_hbm, out_w))
        )
    ]
    for load in loads:
        load.start()
    barrier = pltpu.get_barrier_semaphore()

    def signal(axis, to):
        pl.semaphore_signal(barrier, inc=1, device_id={axis: to}, device_id_type=MESH)

    for bit in bits:
        signal("tp", flip(me, bit))
    for step in steps:
        pl.when(place + step < ep_count)(lambda: signal("ep", place + step))
        pl.when(place >= step)(lambda: signal("ep", place - step))
    peers = sum(
        jnp.where(place + step < ep_count, 1, 0) + jnp.where(place >= step, 1, 0)
        for step in steps
    )
    pl.semaphore_wait(barrier, peers + len(bits))

    exchange = Exchange(tp_count, rows_ref, slots, row_sems)
    exchange.start()
    prefix(ep_count, total_ref, outgoing, incoming, before, send_sem, recv_sem)
    part_width = rows_ref.shape[1]
    units = gate.shape[1]

    def slice_product(block, owner, first):
        at = pl.ds(pl.multiple_of(owner * part_width, part_width), part_width)
        for total, weight in ((gate, gate_w), (up, up_w)):
            product = jnp.dot(block, weight[at, :], preferred_element_type=F32)
            total[...] = product if first else total[...] + product

    loads[0].wait()
    loads[1].wait()
    exchange.relay()
    slice_product(rows_ref[...], me, True)
    columns = read_ref.shape[1]
    groups, width = total_ref.shape[1], total_ref.shape[3]
    ones = head_ones(width)
    for group in range(groups):
        at = pl.ds(group * width, width)
        heads_out = dot(read_ref[:, at], spread(before[1, group])) + local_ref[:, at]
        center = heads_out - dot_exact(heads_out, ones) / HD
        variance = dot_exact(center * center, ones) / HD
        mixed[:, at] = (center * lax.rsqrt(variance + 1.0) * gain_ref[:, at]).astype(BF16)
    for delta in range(1, tp_count):
        exchange.wait(delta)
        slice_product(slots[flip(me, delta)], flip(me, delta), False)
    hidden[...] = (jax.nn.silu(gate[...]) * up[...]).astype(BF16)
    hidden_exchange = Exchange(tp_count, hidden, hidden_slots, hidden_sems)
    hidden_exchange.start()

    def down_product(block, owner):
        at = pl.ds(pl.multiple_of(owner * units, units), units)
        return jnp.dot(block, down_w[at, :], preferred_element_type=F32)

    loads[2].wait()
    loads[3].wait()
    down[...] = down_product(hidden[...], me)
    tile = product_ref.shape[1] // 4
    for number in range(4):
        at = pl.ds(number * tile, tile)
        product_ref[:, at] = jnp.dot(
            mixed[...], out_w[:, at], preferred_element_type=F32
        ).astype(BF16)
        if number == 1:
            hidden_exchange.relay()
    for delta in range(1, tp_count):
        hidden_exchange.wait(delta)
        down[...] += down_product(hidden_slots[flip(me, delta)], flip(me, delta))
    result_ref[...] = (down[...] * share_ref[...]).astype(BF16)
    exchange.finish()
    hidden_exchange.finish()


def experts(rows, gate_w, up_w, down_w, share, total, read, local_out, gain, out_w):
    tp_count, ep_count = lax.axis_size("tp"), lax.axis_size("ep")
    row_count, part_width = rows.shape
    units, out_part = gate_w.shape[1], down_w.shape[1]
    tokens, columns = read.shape
    steps = ep_count.bit_length() - 1
    vmem = pl.BlockSpec(memory_space=pltpu.VMEM)
    hbm = pl.BlockSpec(memory_space=pl.ANY)
    return pl.pallas_call(
        functools.partial(experts_kernel, tp_count, ep_count),
        out_shape=[
            jax.ShapeDtypeStruct((tokens, out_w.shape[1]), BF16),
            jax.ShapeDtypeStruct((row_count, out_part), BF16),
        ],
        in_specs=[vmem, hbm, hbm, hbm, vmem, vmem, vmem, vmem, vmem, hbm],
        out_specs=[vmem, vmem],
        scratch_shapes=[
            pltpu.VMEM((tp_count, row_count, part_width), BF16),
            pltpu.VMEM((tp_count, row_count, units), BF16),
            pltpu.VMEM((row_count, units), BF16),
            pltpu.VMEM(gate_w.shape, BF16),
            pltpu.VMEM(up_w.shape, BF16),
            pltpu.VMEM(down_w.shape, BF16),
            pltpu.VMEM(out_w.shape, BF16),
            pltpu.VMEM((row_count, units), F32),
            pltpu.VMEM((row_count, units), F32),
            pltpu.VMEM((row_count, out_part), F32),
            pltpu.VMEM((tokens, columns), BF16),
            pltpu.VMEM((steps, *total.shape), BF16),
            pltpu.VMEM((steps, *total.shape), BF16),
            pltpu.VMEM(total.shape, F32),
            pltpu.SemaphoreType.DMA((steps,)),
            pltpu.SemaphoreType.DMA((steps,)),
            pltpu.SemaphoreType.DMA((2, 2, tp_count)),
            pltpu.SemaphoreType.DMA((2, 2, tp_count)),
            pltpu.SemaphoreType.DMA((4,)),
        ],
        compiler_params=pltpu.CompilerParams(
            collective_id=0, has_side_effects=True, vmem_limit_bytes=60 * 1024 * 1024
        ),
        name="experts",
    )(rows, gate_w, up_w, down_w, share, total, read, local_out, gain, out_w)


def scatter(product):
    return lax.psum_scatter(product, "tp", scatter_dimension=0, tiled=True)


def return_kernel(count, placed_ref, out_ref, pair_in, held, from_left, from_right, sems):
    me = lax.axis_index("ep")
    chips = count // 2
    core = lax.rem(me, 2)
    chip = me // 2
    partner = me + 1 - 2 * core
    barrier = pltpu.get_barrier_semaphore()

    def signal(to):
        pl.semaphore_signal(barrier, inc=1, device_id={"ep": to}, device_id_type=MESH)

    signal(partner)
    pl.when(chip > 0)(lambda: signal(me - 2))
    pl.when(chip < chips - 1)(lambda: signal(me + 2))
    pl.semaphore_wait(
        barrier, 1 + jnp.where(chip > 0, 1, 0) + jnp.where(chip < chips - 1, 1, 0)
    )

    def send(source, target, kind, slot, to):
        return pltpu.make_async_remote_copy(
            src_ref=source,
            dst_ref=target,
            send_sem=sems.at[kind, 0, slot],
            recv_sem=sems.at[kind, 1, slot],
            device_id={"ep": to},
            device_id_type=MESH,
        )

    order = []
    for step in range(chips):
        order += [at for at in (chips - 1 - step, step) if at not in order]
    pairs = [
        send(placed_ref.at[2 * at + 1 - core], pair_in.at[at], 0, at, partner)
        for at in range(chips)
    ]
    rights = [
        send(from_left.at[at], from_left.at[at], 1, at, jnp.minimum(me + 2, count - 2 + core))
        for at in range(chips)
    ]
    lefts = [
        send(from_right.at[at], from_right.at[at], 2, at, jnp.maximum(me - 2, core))
        for at in range(chips)
    ]
    first_rights = [
        send(held.at[at], from_left.at[at], 1, at, jnp.minimum(me + 2, count - 2 + core))
        for at in range(chips)
    ]
    first_lefts = [
        send(held.at[at], from_right.at[at], 2, at, jnp.maximum(me - 2, core))
        for at in range(chips)
    ]
    for at in order:
        pairs[at].start()

    def pair_sum(at):
        pairs[at].wait_recv()
        held[at] = (
            placed_ref[2 * at + core].astype(F32) + pair_in[at].astype(F32)
        ).astype(BF16)

    def forward(at, moving, first, relay, landing, origin):
        @pl.when(moving & origin)
        def _():
            first.start()

        @pl.when(moving & jnp.logical_not(origin))
        def _():
            relay.wait_recv()
            landing[at] = (landing[at].astype(F32) + held[at].astype(F32)).astype(BF16)
            relay.start()

    ready = []
    for step in range(chips):
        for at in (chips - 1 - step, step):
            if at not in ready:
                pair_sum(at)
                ready.append(at)
        at = chips - 1 - step
        if at > 0:
            forward(at, at > chip, first_rights[at], rights[at], from_left, chip == 0)
        at = step
        if at < chips - 1:
            forward(at, at < chip, first_lefts[at], lefts[at], from_right, chip == chips - 1)
    out_ref[...] = held[chip]

    for at in range(chips):

        @pl.when((at == chip) & (chip > 0))
        def _():
            rights[at].wait_recv()
            out_ref[...] = (out_ref[...].astype(F32) + from_left[at].astype(F32)).astype(BF16)

        @pl.when((at == chip) & (chip < chips - 1))
        def _():
            lefts[at].wait_recv()
            out_ref[...] = (out_ref[...].astype(F32) + from_right[at].astype(F32)).astype(BF16)

    for at in range(chips):
        pairs[at].wait_send()
        pl.when(at > chip)(rights[at].wait_send)
        pl.when(at < chip)(lefts[at].wait_send)


def returned(placed):
    count, rows, width = placed.shape
    chips = count // 2
    vmem = pl.BlockSpec(memory_space=pltpu.VMEM)
    return pl.pallas_call(
        functools.partial(return_kernel, count),
        out_shape=jax.ShapeDtypeStruct((rows, width), BF16),
        in_specs=[vmem],
        out_specs=vmem,
        scratch_shapes=[pltpu.VMEM((chips, rows, width), BF16)] * 4
        + [pltpu.SemaphoreType.DMA((3, 2, chips))],
        compiler_params=pltpu.CompilerParams(collective_id=1, has_side_effects=True),
        name="return",
    )(placed)


def both_halves(
    mixer_args,
    norm_gain,
    out_weight,
    moe_in,
    ffn_gain,
    routes,
    route_weights,
    gate_weight,
    up_weight,
    down_weight,
):
    row_count, feature_count = moe_in.shape
    choose_count = routes.shape[1]
    ep_count = lax.axis_size("ep")
    tp_count = lax.axis_size("tp")
    expert_count = gate_weight.shape[0] * ep_count
    capacity = 5 * row_count * choose_count // (4 * expert_count)
    part_width = feature_count // tp_count
    row_values = moe_in.astype(F32)
    scale = lax.rsqrt(jnp.mean(row_values * row_values, axis=-1, keepdims=True) + 1.0)
    first = lax.axis_index("tp") * part_width
    piece = (
        lax.dynamic_slice_in_dim(moe_in, first, part_width, 1).astype(F32)
        * scale
        * lax.dynamic_slice_in_dim(ffn_gain, first, part_width, 0)
    ).astype(BF16)
    portion = route_weights / jnp.sum(route_weights, axis=-1, keepdims=True)
    names = jnp.arange(expert_count, dtype=jnp.int32)
    table = jnp.sum(
        jnp.where(routes[:, :, None] == names[None, None, :], portion[:, :, None], 0.0), axis=1
    )
    high = table.astype(BF16)
    low = (table - high.astype(F32)).astype(BF16)
    extra = jnp.pad(jnp.concatenate([high, low], axis=1), ((0, 0), (0, 128 - 2 * expert_count)))
    arrived = lax.all_gather(jnp.concatenate([piece, extra], axis=1), "ep")
    tables = block_tables(*mixer_args)
    arrived, (read, local_out, total) = lax.optimization_barrier((arrived, tables))
    mine = lax.axis_index("ep")
    shares = arrived[:, :, part_width:].astype(F32)
    shares = jnp.sum(
        jnp.where(
            lax.broadcasted_iota(jnp.int32, (1, 1, 128), 2) % expert_count == mine, shares, 0.0
        )
        * (lax.broadcasted_iota(jnp.int32, (1, 1, 128), 2) < 2 * expert_count),
        axis=-1,
    )
    named = shares > 0
    earlier = jnp.triu(jnp.ones((row_count, row_count), F32), 1)
    rank = jnp.dot(named.astype(F32), earlier)
    slots = jnp.arange(capacity, dtype=F32)
    chosen = (rank[:, None, :] == slots[None, :, None]) & named[:, None, :]
    onehot = chosen.astype(BF16)
    rows = jnp.einsum(
        "scr,srn->scn", onehot, arrived[:, :, :part_width], preferred_element_type=F32
    ).astype(BF16)
    slot_share = jnp.sum(jnp.where(chosen, shares[:, None, :], 0.0), axis=-1)
    product, result = experts(
        rows.reshape(ep_count * capacity, part_width),
        gate_weight[0],
        up_weight[0],
        down_weight[0],
        slot_share.reshape(ep_count * capacity, 1),
        total,
        read,
        local_out,
        norm_gain[None],
        out_weight,
    )
    placed = jnp.einsum(
        "scr,scd->srd",
        onehot,
        result.reshape(ep_count, capacity, -1),
        preferred_element_type=F32,
    ).astype(BF16)
    return scatter(product), returned(placed)


def local(
    receptance,
    key_in,
    value_in,
    decay_in,
    rate_in,
    norm_gain,
    out_weight,
    moe_in,
    ffn_gain,
    routes,
    route_weights,
    gate_weight,
    up_weight,
    down_weight,
):
    return both_halves(
        (receptance, key_in, value_in, decay_in, rate_in),
        norm_gain,
        out_weight,
        moe_in,
        ffn_gain,
        routes,
        route_weights,
        gate_weight,
        up_weight,
        down_weight,
    )


def solution(mesh):
    return jax.shard_map(
        local,
        mesh=mesh,
        in_specs=(
            P("ep", "tp"),
            P("ep", "tp"),
            P("ep", "tp"),
            P("ep", "tp"),
            P("ep", "tp"),
            P("tp"),
            P("tp", None),
            P("ep", None),
            P(),
            P("ep", None),
            P("ep", None),
            P("ep", None, "tp"),
            P("ep", None, "tp"),
            P("ep", None, "tp"),
        ),
        out_specs=(P(("ep", "tp"), None), P("ep", "tp")),
        check_vma=False,
    )
```

```python
import functools

import jax
import jax.numpy as jnp
from jax import lax
from jax.experimental import pallas as pl
from jax.experimental.pallas import tpu as pltpu
from jax.sharding import PartitionSpec as P

HD = 64
BLOCK = 64
F32 = jnp.float32
BF16 = jnp.bfloat16
MESH = pl.DeviceIdType.MESH


def dot(a, b):
    return jnp.dot(a.astype(BF16), b.astype(BF16), preferred_element_type=F32)


def dot_rows(a, b):
    return lax.dot_general(
        a.astype(BF16), b.astype(BF16), (((1,), (1,)), ((), ())), preferred_element_type=F32
    )


def dot_cols(a, b):
    return lax.dot_general(
        a.astype(BF16), b.astype(BF16), (((0,), (0,)), ((), ())), preferred_element_type=F32
    )


def dot_exact(a, b):
    return jnp.dot(a, b, precision=lax.Precision.HIGHEST, preferred_element_type=F32)


def lane_head(rows, width):
    return lax.broadcasted_iota(jnp.int32, (rows, width), 1) // HD


def spread(packed):
    rows, width = packed.shape
    packed = packed.astype(BF16)
    head = lane_head(rows, width)
    return jnp.concatenate(
        [jnp.where(head == i, packed, jnp.zeros_like(packed)) for i in range(width // HD)], axis=0
    )


def fold(square):
    width = square.shape[1]
    head = lane_head(HD, width)
    out = jnp.zeros((HD, width), F32)
    for i in range(width // HD):
        out = jnp.where(head == i, square[i * HD : (i + 1) * HD], out)
    return out


def head_ones(width):
    row = lax.broadcasted_iota(jnp.int32, (width, width), 0) // HD
    return (row == lane_head(width, width)).astype(F32)


def group_width(columns):
    return HD * max(g for g in (4, 2, 1) if columns % (g * HD) == 0)


def tables_kernel(r_ref, k_ref, v_ref, d_ref, a_ref, read_ref, local_ref, total_ref, carry):
    columns = r_ref.shape[1]
    width = group_width(columns)
    row = lax.broadcasted_iota(jnp.int32, (BLOCK, width), 0)
    lane = lax.broadcasted_iota(jnp.int32, (BLOCK, width), 1) % HD
    strict = lane < row
    closed = lane <= row
    eye = (lane == row).astype(F32)
    tril = (
        lax.broadcasted_iota(jnp.int32, (BLOCK, BLOCK), 1)
        <= lax.broadcasted_iota(jnp.int32, (BLOCK, BLOCK), 0)
    ).astype(F32)
    ones = head_ones(width)

    @pl.when(pl.program_id(0) == 0)
    def _():
        for group in range(columns // width):
            carry[0, group] = eye
            carry[1, group] = jnp.zeros_like(eye)

    for group in range(columns // width):
        at = pl.ds(group * width, width)
        readout = r_ref[:, at].astype(F32)
        key = k_ref[:, at].astype(F32)
        value = v_ref[:, at]
        log_decay = jax.nn.sigmoid(d_ref[:, at].astype(F32)) * -0.6065306597126334
        rate = jax.nn.sigmoid(a_ref[:, at].astype(F32))
        unit = key * lax.rsqrt(dot_exact(key * key, ones) + 1.0)
        inclusive = dot_exact(tril, log_decay)
        total = inclusive[BLOCK - 1 :]
        probe = -unit * jnp.exp(inclusive - log_decay)
        removal = unit * rate
        written = key * rate
        back = jnp.exp(-inclusive)
        tail = jnp.exp(total - inclusive)
        readout = readout * jnp.exp(inclusive)
        left = jnp.concatenate([probe, readout], axis=0)
        on_removal = dot_rows(left, spread(removal * back))
        on_write = dot_rows(left, spread(written * back))
        lower = jnp.where(strict, on_removal[:BLOCK], 0.0)
        reach = jnp.where(closed, on_removal[BLOCK:], 0.0)
        lower_write = jnp.where(strict, on_write[:BLOCK], 0.0)
        reach_write = jnp.where(closed, on_write[BLOCK:], 0.0)
        value_wide = spread(value)
        on_value = dot(jnp.concatenate([lower_write, reach_write], axis=0), value_wide)
        inverse = eye + lower
        power = dot(lower, spread(lower))
        for doubling in range(BLOCK.bit_length() - 2):
            wide = spread(power)
            if doubling < BLOCK.bit_length() - 3:
                both = dot(jnp.concatenate([inverse, power], axis=0), wide)
                inverse = inverse + both[:BLOCK]
                power = both[BLOCK:]
            else:
                inverse = inverse + dot(inverse, wide)
        solved_probe = dot(inverse, spread(probe))
        solved_values = dot(inverse, spread(on_value[:BLOCK]))
        transition = eye * jnp.exp(total) + fold(dot_cols(removal * tail, solved_probe))
        increment = fold(
            dot_cols(
                jnp.concatenate([removal * tail, written * tail], axis=0),
                jnp.concatenate([solved_values.astype(BF16), value], axis=0),
            )
        )
        read_state = readout + dot(reach, spread(solved_probe))
        local_out = dot(reach, spread(solved_values)) + on_value[BLOCK:]
        left = jnp.concatenate([read_state, transition], axis=0)
        on_map = dot(left, spread(carry[0, group]))
        on_add = dot(left, spread(carry[1, group]))
        read_ref[:, at] = on_map[:BLOCK].astype(BF16)
        local_ref[:, at] = on_add[:BLOCK] + local_out
        carry[0, group] = on_map[BLOCK:]
        carry[1, group] = on_add[BLOCK:] + increment
        total_ref[0, group] = on_map[BLOCK:].astype(BF16)
        total_ref[1, group] = (on_add[BLOCK:] + increment).astype(BF16)


def block_tables(receptance, key_in, value_in, decay_in, rate_in):
    tokens, columns = receptance.shape
    width = group_width(columns)
    groups = columns // width
    rows = pl.BlockSpec((BLOCK, columns), lambda b: (b, 0))
    return pl.pallas_call(
        tables_kernel,
        grid=(tokens // BLOCK,),
        in_specs=[rows] * 5,
        out_specs=[rows, rows, pl.BlockSpec((2, groups, HD, width), lambda b: (0, 0, 0, 0))],
        out_shape=[
            jax.ShapeDtypeStruct((tokens, columns), BF16),
            jax.ShapeDtypeStruct((tokens, columns), F32),
            jax.ShapeDtypeStruct((2, groups, HD, width), BF16),
        ],
        scratch_shapes=[pltpu.VMEM((2, groups, HD, width), F32)],
        name="tables",
    )(receptance, key_in, value_in, decay_in, rate_in)


def flip(me, bits):
    bit = 1
    while bit <= bits:
        if bits & bit:
            me = me + bit - 2 * bit * ((me // bit) % 2)
        bit *= 2
    return me


class Exchange:
    def __init__(self, count, own, slots, sems):
        me = lax.axis_index("tp")
        half = own.shape[0] // 2
        bits = [1 << b for b in range(count.bit_length() - 1)]
        self.count, self.copies, self.heads, self.relays, self.seen = count, {}, [], [], set()
        for number in range(len(bits)):
            for stream, order in enumerate((bits, bits[::-1])):
                at = pl.ds(stream * half, half)
                known = [0]
                for bit in order[:number]:
                    known += [k ^ bit for k in known]
                for from_delta in known:
                    bit = order[number]
                    key = (stream, from_delta ^ bit)
                    owner = flip(me, from_delta)
                    self.copies[key] = pltpu.make_async_remote_copy(
                        src_ref=slots.at[owner, at] if from_delta else own.at[at],
                        dst_ref=slots.at[owner, at],
                        send_sem=sems.at[0, stream, key[1]],
                        recv_sem=sems.at[1, stream, key[1]],
                        device_id={"tp": flip(me, bit)},
                        device_id_type=MESH,
                    )
                    if from_delta:
                        self.relays.append((key, from_delta))
                    else:
                        self.heads.append(key)

    def start(self):
        for key in self.heads:
            self.copies[key].start()

    def arrive(self, stream, delta):
        if (stream, delta) not in self.seen:
            self.seen.add((stream, delta))
            self.copies[stream, delta].wait_recv()

    def relay(self):
        for key, from_delta in self.relays:
            self.arrive(key[0], from_delta)
            self.copies[key].start()

    def wait(self, delta):
        for stream in (0, 1):
            self.arrive(stream, delta)

    def finish(self):
        for copy in self.copies.values():
            copy.wait_send()


def prefix(count, own_ref, outgoing, incoming, before, send_sem, recv_sem):
    me = lax.axis_index("ep")
    groups = own_ref.shape[1]
    steps = [1 << s for s in range(count.bit_length() - 1)]
    width = own_ref.shape[3]
    lane = lax.broadcasted_iota(jnp.int32, (HD, width), 1) % HD
    eye = (lane == lax.broadcasted_iota(jnp.int32, (HD, width), 0)).astype(F32)
    for group in range(groups):
        before[0, group] = eye
        before[1, group] = jnp.zeros_like(eye)
    for number, step in enumerate(steps):
        last = number == len(steps) - 1
        source = own_ref if number == 0 else outgoing.at[number - 1]
        target = incoming.at[number]
        if last:
            source, target = source.at[1], target.at[1]
        copy = pltpu.make_async_remote_copy(
            src_ref=source,
            dst_ref=target,
            send_sem=send_sem.at[number],
            recv_sem=recv_sem.at[number],
            device_id={"ep": lax.rem(me + step, count)},
            device_id_type=MESH,
        )

        @pl.when(me + step < count)
        def _():
            copy.start()

        @pl.when(me >= step)
        def _():
            copy.wait_recv()
            for group in range(groups):
                left = before[0, group]
                before[1, group] += dot(left, spread(incoming[number, 1, group]))
                if not last:
                    before[0, group] = dot(left, spread(incoming[number, 0, group]))

        if not last:
            for group in range(groups):
                left = own_ref[0, group]
                outgoing[number, 0, group] = dot(left, spread(before[0, group])).astype(BF16)
                outgoing[number, 1, group] = (
                    dot(left, spread(before[1, group])) + own_ref[1, group].astype(F32)
                ).astype(BF16)

        @pl.when(me + step < count)
        def _():
            copy.wait_send()


def experts_kernel(
    tp_count,
    ep_count,
    rows_ref,
    gate_hbm,
    up_hbm,
    down_hbm,
    share_ref,
    total_ref,
    read_ref,
    local_ref,
    gain_ref,
    weight_hbm,
    product_ref,
    result_ref,
    slots,
    hidden_slots,
    hidden,
    gate_w,
    up_w,
    down_w,
    out_w,
    gate,
    up,
    down,
    mixed,
    outgoing,
    incoming,
    before,
    send_sem,
    recv_sem,
    row_sems,
    hidden_sems,
    load_sems,
):
    me = lax.axis_index("tp")
    place = lax.axis_index("ep")
    steps = [1 << s for s in range(ep_count.bit_length() - 1)]
    bits = [1 << b for b in range(tp_count.bit_length() - 1)]
    loads = [
        pltpu.make_async_copy(source, target, load_sems.at[i])
        for i, (source, target) in enumerate(
            ((gate_hbm, gate_w), (up_hbm, up_w), (down_hbm, down_w), (weight_hbm, out_w))
        )
    ]
    for load in loads:
        load.start()
    barrier = pltpu.get_barrier_semaphore()

    def signal(axis, to):
        pl.semaphore_signal(barrier, inc=1, device_id={axis: to}, device_id_type=MESH)

    for bit in bits:
        signal("tp", flip(me, bit))
    for step in steps:
        pl.when(place + step < ep_count)(lambda: signal("ep", place + step))
        pl.when(place >= step)(lambda: signal("ep", place - step))
    peers = sum(
        jnp.where(place + step < ep_count, 1, 0) + jnp.where(place >= step, 1, 0)
        for step in steps
    )
    pl.semaphore_wait(barrier, peers + len(bits))

    exchange = Exchange(tp_count, rows_ref, slots, row_sems)
    exchange.start()
    prefix(ep_count, total_ref, outgoing, incoming, before, send_sem, recv_sem)
    part_width = rows_ref.shape[1]
    units = gate.shape[1]

    def slice_product(block, owner, first):
        at = pl.ds(pl.multiple_of(owner * part_width, part_width), part_width)
        for total, weight in ((gate, gate_w), (up, up_w)):
            product = jnp.dot(block, weight[at, :], preferred_element_type=F32)
            total[...] = product if first else total[...] + product

    loads[0].wait()
    loads[1].wait()
    exchange.relay()
    slice_product(rows_ref[...], me, True)
    columns = read_ref.shape[1]
    groups, width = total_ref.shape[1], total_ref.shape[3]
    ones = head_ones(width)
    for group in range(groups):
        at = pl.ds(group * width, width)
        heads_out = dot(read_ref[:, at], spread(before[1, group])) + local_ref[:, at]
        center = heads_out - dot_exact(heads_out, ones) / HD
        variance = dot_exact(center * center, ones) / HD
        mixed[:, at] = (center * lax.rsqrt(variance + 1.0) * gain_ref[:, at]).astype(BF16)
    for delta in range(1, tp_count):
        exchange.wait(delta)
        slice_product(slots[flip(me, delta)], flip(me, delta), False)
    hidden[...] = (jax.nn.silu(gate[...]) * up[...]).astype(BF16)
    hidden_exchange = Exchange(tp_count, hidden, hidden_slots, hidden_sems)
    hidden_exchange.start()

    def down_product(block, owner):
        at = pl.ds(pl.multiple_of(owner * units, units), units)
        return jnp.dot(block, down_w[at, :], preferred_element_type=F32)

    loads[2].wait()
    loads[3].wait()
    down[...] = down_product(hidden[...], me)
    tile = product_ref.shape[1] // 4
    for number in range(4):
        at = pl.ds(number * tile, tile)
        product_ref[:, at] = jnp.dot(
            mixed[...], out_w[:, at], preferred_element_type=F32
        ).astype(BF16)
        if number == 1:
            hidden_exchange.relay()
    for delta in range(1, tp_count):
        hidden_exchange.wait(delta)
        down[...] += down_product(hidden_slots[flip(me, delta)], flip(me, delta))
    result_ref[...] = (down[...] * share_ref[...]).astype(BF16)
    exchange.finish()
    hidden_exchange.finish()


def experts(rows, gate_w, up_w, down_w, share, total, read, local_out, gain, out_w):
    tp_count, ep_count = lax.axis_size("tp"), lax.axis_size("ep")
    row_count, part_width = rows.shape
    units, out_part = gate_w.shape[1], down_w.shape[1]
    tokens, columns = read.shape
    steps = ep_count.bit_length() - 1
    vmem = pl.BlockSpec(memory_space=pltpu.VMEM)
    hbm = pl.BlockSpec(memory_space=pl.ANY)
    return pl.pallas_call(
        functools.partial(experts_kernel, tp_count, ep_count),
        out_shape=[
            jax.ShapeDtypeStruct((tokens, out_w.shape[1]), BF16),
            jax.ShapeDtypeStruct((row_count, out_part), BF16),
        ],
        in_specs=[vmem, hbm, hbm, hbm, vmem, vmem, vmem, vmem, vmem, hbm],
        out_specs=[vmem, vmem],
        scratch_shapes=[
            pltpu.VMEM((tp_count, row_count, part_width), BF16),
            pltpu.VMEM((tp_count, row_count, units), BF16),
            pltpu.VMEM((row_count, units), BF16),
            pltpu.VMEM(gate_w.shape, BF16),
            pltpu.VMEM(up_w.shape, BF16),
            pltpu.VMEM(down_w.shape, BF16),
            pltpu.VMEM(out_w.shape, BF16),
            pltpu.VMEM((row_count, units), F32),
            pltpu.VMEM((row_count, units), F32),
            pltpu.VMEM((row_count, out_part), F32),
            pltpu.VMEM((tokens, columns), BF16),
            pltpu.VMEM((steps, *total.shape), BF16),
            pltpu.VMEM((steps, *total.shape), BF16),
            pltpu.VMEM(total.shape, F32),
            pltpu.SemaphoreType.DMA((steps,)),
            pltpu.SemaphoreType.DMA((steps,)),
            pltpu.SemaphoreType.DMA((2, 2, tp_count)),
            pltpu.SemaphoreType.DMA((2, 2, tp_count)),
            pltpu.SemaphoreType.DMA((4,)),
        ],
        compiler_params=pltpu.CompilerParams(
            collective_id=0, has_side_effects=True, vmem_limit_bytes=60 * 1024 * 1024
        ),
        name="experts",
    )(rows, gate_w, up_w, down_w, share, total, read, local_out, gain, out_w)


def scatter(product):
    return lax.psum_scatter(product, "tp", scatter_dimension=0, tiled=True)


def return_kernel(count, placed_ref, out_ref, pair_in, held, from_left, from_right, sems):
    me = lax.axis_index("ep")
    chips = count // 2
    core = lax.rem(me, 2)
    chip = me // 2
    partner = me + 1 - 2 * core
    barrier = pltpu.get_barrier_semaphore()

    def signal(to):
        pl.semaphore_signal(barrier, inc=1, device_id={"ep": to}, device_id_type=MESH)

    signal(partner)
    pl.when(chip > 0)(lambda: signal(me - 2))
    pl.when(chip < chips - 1)(lambda: signal(me + 2))
    pl.semaphore_wait(
        barrier, 1 + jnp.where(chip > 0, 1, 0) + jnp.where(chip < chips - 1, 1, 0)
    )

    half = out_ref.shape[0] // 2
    right_to = jnp.minimum(me + 2, count - 2 + core)
    left_to = jnp.maximum(me - 2, core)

    def send(source, target, kind, item, to):
        at, part = item
        rows = pl.ds(part * half, half)
        return pltpu.make_async_remote_copy(
            src_ref=source.at[rows],
            dst_ref=target.at[at, rows],
            send_sem=sems.at[kind, 0, 2 * at + part],
            recv_sem=sems.at[kind, 1, 2 * at + part],
            device_id={"ep": to},
            device_id_type=MESH,
        )

    def pair(item):
        return send(placed_ref.at[2 * item[0] + 1 - core], pair_in, 0, item, partner)

    def right(item, source=from_left):
        return send(source.at[item[0]], from_left, 1, item, right_to)

    def left(item, source=from_right):
        return send(source.at[item[0]], from_right, 2, item, left_to)

    order = []
    for step in range(chips):
        order += [at for at in (chips - 1 - step, step) if at not in order]
    items = [(at, part) for at in order for part in (0, 1)]
    for item in items:
        pair(item).start()

    def pair_sum(item):
        at, part = item
        rows = pl.ds(part * half, half)
        pair(item).wait_recv()
        held[at, rows] = (
            placed_ref[2 * at + core, rows].astype(F32) + pair_in[at, rows].astype(F32)
        ).astype(BF16)

    def forward(item, moving, hop, landing, origin):
        at, part = item
        rows = pl.ds(part * half, half)

        @pl.when(moving & origin)
        def _():
            hop(item, held).start()

        @pl.when(moving & jnp.logical_not(origin))
        def _():
            relay = hop(item)
            relay.wait_recv()
            landing[at, rows] = (
                landing[at, rows].astype(F32) + held[at, rows].astype(F32)
            ).astype(BF16)
            relay.start()

    ready = []
    for step in range(chips):
        for at in (chips - 1 - step, step):
            if at not in ready:
                pair_sum((at, 0))
                pair_sum((at, 1))
                ready.append(at)
        for part in (0, 1):

            def rightward(at=chips - 1 - step, part=part):
                if at > 0:
                    forward((at, part), at > chip, right, from_left, chip == 0)

            def leftward(at=step, part=part):
                if at < chips - 1:
                    forward((at, part), at < chip, left, from_right, chip == chips - 1)

            @pl.when(chip < chips // 2)
            def _():
                rightward()
                leftward()

            @pl.when(chip >= chips // 2)
            def _():
                leftward()
                rightward()

    for at in range(chips):

        @pl.when(at == chip)
        def _():
            for part in (0, 1):
                rows = pl.ds(part * half, half)
                out_ref[rows] = held[at, rows]

                @pl.when(chip > 0)
                def _():
                    right((at, part)).wait_recv()
                    out_ref[rows] = (
                        out_ref[rows].astype(F32) + from_left[at, rows].astype(F32)
                    ).astype(BF16)

                @pl.when(chip < chips - 1)
                def _():
                    left((at, part)).wait_recv()
                    out_ref[rows] = (
                        out_ref[rows].astype(F32) + from_right[at, rows].astype(F32)
                    ).astype(BF16)

    for item in items:
        pair(item).wait_send()
        pl.when(item[0] > chip)(lambda: right(item).wait_send())
        pl.when(item[0] < chip)(lambda: left(item).wait_send())


def returned(placed):
    count, rows, width = placed.shape
    chips = count // 2
    vmem = pl.BlockSpec(memory_space=pltpu.VMEM)
    return pl.pallas_call(
        functools.partial(return_kernel, count),
        out_shape=jax.ShapeDtypeStruct((rows, width), BF16),
        in_specs=[vmem],
        out_specs=vmem,
        scratch_shapes=[pltpu.VMEM((chips, rows, width), BF16)] * 4
        + [pltpu.SemaphoreType.DMA((3, 2, 2 * chips))],
        compiler_params=pltpu.CompilerParams(collective_id=1, has_side_effects=True),
        name="return",
    )(placed)


def both_halves(
    mixer_args,
    norm_gain,
    out_weight,
    moe_in,
    ffn_gain,
    routes,
    route_weights,
    gate_weight,
    up_weight,
    down_weight,
):
    row_count, feature_count = moe_in.shape
    choose_count = routes.shape[1]
    ep_count = lax.axis_size("ep")
    tp_count = lax.axis_size("tp")
    expert_count = gate_weight.shape[0] * ep_count
    capacity = 5 * row_count * choose_count // (4 * expert_count)
    part_width = feature_count // tp_count
    row_values = moe_in.astype(F32)
    scale = lax.rsqrt(jnp.mean(row_values * row_values, axis=-1, keepdims=True) + 1.0)
    first = lax.axis_index("tp") * part_width
    piece = (
        lax.dynamic_slice_in_dim(moe_in, first, part_width, 1).astype(F32)
        * scale
        * lax.dynamic_slice_in_dim(ffn_gain, first, part_width, 0)
    ).astype(BF16)
    portion = route_weights / jnp.sum(route_weights, axis=-1, keepdims=True)
    names = jnp.arange(expert_count, dtype=jnp.int32)
    table = jnp.sum(
        jnp.where(routes[:, :, None] == names[None, None, :], portion[:, :, None], 0.0), axis=1
    )
    high = table.astype(BF16)
    low = (table - high.astype(F32)).astype(BF16)
    extra = jnp.pad(jnp.concatenate([high, low], axis=1), ((0, 0), (0, 128 - 2 * expert_count)))
    arrived = lax.all_gather(jnp.concatenate([piece, extra], axis=1), "ep")
    tables = block_tables(*mixer_args)
    arrived, (read, local_out, total) = lax.optimization_barrier((arrived, tables))
    mine = lax.axis_index("ep")
    shares = arrived[:, :, part_width:].astype(F32)
    shares = jnp.sum(
        jnp.where(
            lax.broadcasted_iota(jnp.int32, (1, 1, 128), 2) % expert_count == mine, shares, 0.0
        )
        * (lax.broadcasted_iota(jnp.int32, (1, 1, 128), 2) < 2 * expert_count),
        axis=-1,
    )
    named = shares > 0
    earlier = jnp.triu(jnp.ones((row_count, row_count), F32), 1)
    rank = jnp.dot(named.astype(F32), earlier)
    slots = jnp.arange(capacity, dtype=F32)
    chosen = (rank[:, None, :] == slots[None, :, None]) & named[:, None, :]
    onehot = chosen.astype(BF16)
    rows = jnp.einsum(
        "scr,srn->scn", onehot, arrived[:, :, :part_width], preferred_element_type=F32
    ).astype(BF16)
    slot_share = jnp.sum(jnp.where(chosen, shares[:, None, :], 0.0), axis=-1)
    product, result = experts(
        rows.reshape(ep_count * capacity, part_width),
        gate_weight[0],
        up_weight[0],
        down_weight[0],
        slot_share.reshape(ep_count * capacity, 1),
        total,
        read,
        local_out,
        norm_gain[None],
        out_weight,
    )
    placed = jnp.einsum(
        "scr,scd->srd",
        onehot,
        result.reshape(ep_count, capacity, -1),
        preferred_element_type=F32,
    ).astype(BF16)
    return scatter(product), returned(placed)


def local(
    receptance,
    key_in,
    value_in,
    decay_in,
    rate_in,
    norm_gain,
    out_weight,
    moe_in,
    ffn_gain,
    routes,
    route_weights,
    gate_weight,
    up_weight,
    down_weight,
):
    return both_halves(
        (receptance, key_in, value_in, decay_in, rate_in),
        norm_gain,
        out_weight,
        moe_in,
        ffn_gain,
        routes,
        route_weights,
        gate_weight,
        up_weight,
        down_weight,
    )


def solution(mesh):
    return jax.shard_map(
        local,
        mesh=mesh,
        in_specs=(
            P("ep", "tp"),
            P("ep", "tp"),
            P("ep", "tp"),
            P("ep", "tp"),
            P("ep", "tp"),
            P("tp"),
            P("tp", None),
            P("ep", None),
            P(),
            P("ep", None),
            P("ep", None),
            P("ep", None, "tp"),
            P("ep", None, "tp"),
            P("ep", None, "tp"),
        ),
        out_specs=(P(("ep", "tp"), None), P("ep", "tp")),
        check_vma=False,
    )
```
